32 devices in a mesh: sp: 8 (over z, y), tp: 4 (over x, core).
Axes of the slice: x: 2, y: 2, z: 4, core: 2. Of those that a mesh axis runs over, the one named last changes fastest.
Arguments:
- resid: bfloat16 [2048, 2048], P(('sp', 'tp')), may hold values from -0.3125 to 0.3125
- q_latent: bfloat16 [2048, 768], P('sp'), may hold values from -6 to 6
- kv_latent: bfloat16 [2048, 512], P('sp'), may hold values from -6 to 6
- rope_key: bfloat16 [2048, 32], P('sp'), may hold values from -6 to 6
- q_gain: float32 [768], replicated, may hold values from 0.6 to 10, as said below
- kv_gain: float32 [512], replicated, may hold values from 0.6 to 10
- w_q_small: bfloat16 [768, 768], P(None, 'tp'), may hold values from -0.21875 to 0.21875
- w_q_large: bfloat16 [768, 1280], P(None, 'tp'), may hold values from -0.21875 to 0.21875
- w_kv_small: bfloat16 [512, 1024], P(None, 'tp'), may hold values from -0.25 to 0.25
- w_kv_large: bfloat16 [512, 2048], P(None, 'tp'), may hold values from -0.25 to 0.25
- w_out_small: bfloat16 [512, 2048], P('tp'), may hold values from -0.15625 to 0.15625
- w_out_large: bfloat16 [1024, 2048], P('tp'), may hold values from -0.15625 to 0.15625
- ffn_gain: float32 [2048], replicated, may hold values from 0.1 to 1.9
- w_up: bfloat16 [2048, 8192], P('sp', 'tp'), may hold values from -0.125 to 0.125
- w_down: bfloat16 [8192, 2048], P('tp', 'sp'), may hold values from -0.0625 to 0.0625
Outputs:
- layer_out: bfloat16 [2048, 2048], P(('sp', 'tp'))
The draws below stay inside these ranges and needn't reach their ends.
Inputs may be any that keep to these rules, and one draw needn't show every extreme that they name: q_gain and kv_gain are positive.
All inputs are finite; a program needn't handle non-finite values.
Results may differ from the reference program's by a relative error of at most 0.025.
The reference program's roundings to bfloat16 on the way (of `query_normed`, `key_normed`, `key_rot`, `weights`, `after_attn`, `ffn_normed` and `hidden`) count: a program that leaves them out, or rounds other values in their place, can miss the bound.
Values may be sent and summed in bfloat16 or wider, within the bound.
A program may use at most 128 MiB of HBM per device.

```python
import math
import jax
import jax.numpy as jnp
from jax import lax

WIDTH = 2048
MIXER_UNITS = 8192
QUERY_RANK = 768
LATENT_RANK = 512
HEADS_SMALL = 8
HEADS_LARGE = 8
SMALL_DIM = 64
LARGE_DIM = 128
ROPE_DIM = 32
TOKENS = 2048


def draw_q_gain(key, part):
    return jnp.exp(jax.random.uniform(key, (QUERY_RANK,), jnp.float32, -0.4, 0.4))


def draw_kv_gain(key, part):
    return jnp.exp(jax.random.uniform(key, (LATENT_RANK,), jnp.float32, -0.4, 0.4))


def block_levels(own_key, shape, shards, low, largest):
    factor_of, own = 1.0, jax.random.fold_in(own_key, 6)
    for position, shards_of in shards:
        heights = jnp.exp(jax.random.uniform(jax.random.fold_in(own, position), (shards_of,), jnp.float32, low / len(shards), largest / len(shards)))
        factor_of = factor_of * jnp.repeat(heights, shape[position] // shards_of).reshape([-1 if axis == position else 1 for axis in range(len(shape))])
    return factor_of


def normal_values(own_key, dims, width, limit, cuts=(), held_as=jnp.bfloat16):
    values = width * jax.random.normal(own_key, dims, jnp.float32)
    if cuts:
        values = values * block_levels(own_key, dims, cuts, -0.22, 0.18)
    return jnp.clip(values, -limit, limit).astype(held_as)


def setup_inputs(seed: int = 0) -> dict:
    arg_keys = jax.random.split(jax.random.key(seed), 16)
    return {
        "resid": normal_values(arg_keys[0], (TOKENS, WIDTH), 0.02, 0.3125, ((0, 32),)),
        "q_latent": normal_values(arg_keys[1], (TOKENS, QUERY_RANK), 1.0, 6.0, ((0, 8),)),
        "kv_latent": normal_values(arg_keys[2], (TOKENS, LATENT_RANK), 1.0, 6.0, ((0, 8),)),
        "rope_key": normal_values(arg_keys[3], (TOKENS, ROPE_DIM), 1.0, 6.0, ((0, 8),)),
        "q_gain": draw_q_gain(jax.random.fold_in(arg_keys[15], 71), 0),
        "kv_gain": draw_kv_gain(jax.random.fold_in(arg_keys[15], 71), 0),
        "w_q_small": normal_values(arg_keys[6], (QUERY_RANK, HEADS_SMALL * (SMALL_DIM + ROPE_DIM)), QUERY_RANK ** -0.5, 0.21875, ((1, 4),)),
        "w_q_large": normal_values(arg_keys[7], (QUERY_RANK, HEADS_LARGE * (LARGE_DIM + ROPE_DIM)), QUERY_RANK ** -0.5, 0.21875, ((1, 4),)),
        "w_kv_small": normal_values(arg_keys[8], (LATENT_RANK, HEADS_SMALL * 2 * SMALL_DIM), LATENT_RANK ** -0.5, 0.25, ((1, 4),)),
        "w_kv_large": normal_values(arg_keys[9], (LATENT_RANK, HEADS_LARGE * 2 * LARGE_DIM), LATENT_RANK ** -0.5, 0.25, ((1, 4),)),
        "w_out_small": normal_values(arg_keys[10], (HEADS_SMALL * SMALL_DIM, WIDTH), (HEADS_SMALL * SMALL_DIM + HEADS_LARGE * LARGE_DIM) ** -0.5, 0.15625, ((0, 4),)),
        "w_out_large": normal_values(arg_keys[11], (HEADS_LARGE * LARGE_DIM, WIDTH), (HEADS_SMALL * SMALL_DIM + HEADS_LARGE * LARGE_DIM) ** -0.5, 0.15625, ((0, 4),)),
        "ffn_gain": jnp.clip(1.0 + 0.18 * jax.random.normal(arg_keys[12], (WIDTH,), jnp.float32), 0.1, 1.9),
        "w_up": normal_values(arg_keys[13], (WIDTH, MIXER_UNITS), WIDTH ** -0.5, 0.125, ((0, 8), (1, 4))),
        "w_down": normal_values(arg_keys[14], (MIXER_UNITS, WIDTH), MIXER_UNITS ** -0.5, 0.0625, ((0, 4), (1, 8))),
    }


epsilon = 1e-06
theta_base = 10000.0

def rms_scale(inputs, gain_vec):
    values = inputs.astype(jnp.float32)
    return values * lax.rsqrt(lax.optimization_barrier(jnp.mean(values * values, axis=-1, keepdims=True)) + epsilon) * gain_vec

def rotary(values, positions):
    halfway = values.shape[-1] // 2
    inverse = theta_base ** (-jnp.arange(0, 2 * halfway, 2, dtype=jnp.float32) / (2 * halfway))
    angles = positions.astype(jnp.float32)[:, None] * inverse[None, :]
    cos_table = jnp.cos(angles)
    sin_table = jnp.sin(angles)
    if values.ndim == 3:
        cos_table = cos_table[:, None, :]
        sin_table = sin_table[:, None, :]
    first_half = values[..., :halfway]
    second_half = values[..., halfway:]
    return jnp.concatenate([first_half * cos_table - second_half * sin_table, second_half * cos_table + first_half * sin_table], axis=-1)

def queries(normed, weight, nope_dim, positions):
    projected = jnp.dot(normed, weight, preferred_element_type=jnp.float32)
    projected = projected.reshape(projected.shape[0], -1, nope_dim + ROPE_DIM)
    turned = rotary(projected[..., nope_dim:], positions)
    return jnp.concatenate([projected[..., :nope_dim], turned], axis=-1).astype(jnp.bfloat16)

def group_attention(query_rows, keys_values, key_rot, nope_dim):
    length = query_rows.shape[0]
    head_count = query_rows.shape[1]
    block_rows = math.gcd(length, 512)
    block_count = length // block_rows
    key_part = keys_values[..., :nope_dim].astype(jnp.float32)
    value_part = keys_values[..., nope_dim:].astype(jnp.float32)
    rot_f32 = key_rot.astype(jnp.float32)
    score_scale = (nope_dim + ROPE_DIM) ** (-0.5)
    key_pos = jnp.arange(length, dtype=jnp.int32)

    def attend_block(block_args):
        query_block, block_index = block_args
        query_f32 = query_block.astype(jnp.float32)
        scores = jnp.einsum('qhd,khd->hqk', query_f32[..., :nope_dim], key_part)
        scores = scores + jnp.einsum('qhr,kr->hqk', query_f32[..., nope_dim:], rot_f32)
        scores = scores * score_scale
        query_pos = block_index * block_rows + jnp.arange(block_rows, dtype=jnp.int32)
        causal = key_pos[None, :] <= query_pos[:, None]
        scores = jnp.where(causal[None], scores, -jnp.inf)
        row_max = lax.optimization_barrier(jnp.max(scores, axis=-1, keepdims=True))
        exponent = jnp.exp(scores - row_max)
        row_sum = lax.optimization_barrier(jnp.sum(exponent, axis=-1))
        weights = lax.optimization_barrier(exponent.astype(jnp.bfloat16)).astype(jnp.float32)
        summed = jnp.einsum('hqk,khd->qhd', weights, value_part)
        return (summed / jnp.transpose(row_sum)[:, :, None]).astype(jnp.bfloat16)
    blocks = query_rows.reshape(block_count, block_rows, head_count, query_rows.shape[-1])
    result = lax.map(attend_block, (blocks, jnp.arange(block_count, dtype=jnp.int32)))
    return result.reshape(length, -1)

def reference(resid, q_latent, kv_latent, rope_key, q_gain, kv_gain, w_q_small, w_q_large, w_kv_small, w_kv_large, w_out_small, w_out_large, ffn_gain, w_up, w_down):
    positions = jnp.arange(TOKENS, dtype=jnp.int32)
    query_normed = rms_scale(q_latent, q_gain).astype(jnp.bfloat16)
    key_normed = rms_scale(kv_latent, kv_gain).astype(jnp.bfloat16)
    key_rot = rotary(rope_key.astype(jnp.float32), positions).astype(jnp.bfloat16)
    query_small = queries(query_normed, w_q_small, SMALL_DIM, positions)
    query_large = queries(query_normed, w_q_large, LARGE_DIM, positions)
    kv_small = jnp.dot(key_normed, w_kv_small, preferred_element_type=jnp.float32).astype(jnp.bfloat16)
    kv_small = kv_small.reshape(TOKENS, HEADS_SMALL, 2 * SMALL_DIM)
    kv_large = jnp.dot(key_normed, w_kv_large, preferred_element_type=jnp.float32).astype(jnp.bfloat16)
    kv_large = kv_large.reshape(TOKENS, HEADS_LARGE, 2 * LARGE_DIM)
    attn_small = group_attention(query_small, kv_small, key_rot, SMALL_DIM)
    attn_large = group_attention(query_large, kv_large, key_rot, LARGE_DIM)
    mixed_rows = jnp.dot(attn_small, w_out_small, preferred_element_type=jnp.float32)
    mixed_rows = mixed_rows + jnp.dot(attn_large, w_out_large, preferred_element_type=jnp.float32)
    after_attn = (resid.astype(jnp.float32) + mixed_rows).astype(jnp.bfloat16)
    ffn_normed = rms_scale(after_attn, ffn_gain).astype(jnp.bfloat16)
    hidden = jnp.square(jax.nn.relu(jnp.dot(ffn_normed, w_up, preferred_element_type=jnp.float32)))
    hidden = hidden.astype(jnp.bfloat16)
    ffn_rows = jnp.dot(hidden, w_down, preferred_element_type=jnp.float32)
    return (after_attn.astype(jnp.float32) + ffn_rows).astype(jnp.bfloat16)
```

```python
import functools

import jax
import jax.numpy as jnp
from jax import lax
from jax.experimental import pallas as pl
from jax.experimental.pallas import tpu as pltpu
from jax.sharding import PartitionSpec as P

SMALL_DIM = 64
LARGE_DIM = 128
ROPE_DIM = 32
HALF_ROPE = ROPE_DIM // 2

epsilon = 1e-06
theta_base = 10000.0
LOG2E = 1.4426950408889634

MESH = pl.DeviceIdType.MESH
CORES = 2
LANES = 128
HALVES = 2


def rms_scale(inputs, gain_vec):
    values = inputs.astype(jnp.float32)
    return (
        values * lax.rsqrt(jnp.mean(values * values, axis=-1, keepdims=True) + epsilon) * gain_vec
    )


def rotary_tables(positions):
    lane = jnp.arange(LANES, dtype=jnp.int32)
    exponent = (2 * (lane % HALF_ROPE)).astype(jnp.float32) / ROPE_DIM
    angles = positions.astype(jnp.float32)[:, None] * (theta_base ** (-exponent))[None, :]
    inside = (lane < ROPE_DIM)[None, :]
    sign = jnp.where(lane < HALF_ROPE, -1.0, 1.0)[None, :]
    return jnp.where(inside, jnp.cos(angles), 0.0), jnp.where(inside, sign * jnp.sin(angles), 0.0)


def inner_split(count):
    best = 1
    for size in range(1, count + 1):
        if size * size <= count and count % size == 0:
            best = size
    return best


def near_first(count):
    return sorted(range(1, count), key=lambda k: (min(k, count - k), k))


def remote(src, dst, send_sem, recv_sem, device):
    return pltpu.make_async_remote_copy(
        src_ref=src,
        dst_ref=dst,
        send_sem=send_sem,
        recv_sem=recv_sem,
        device_id=device,
        device_id_type=MESH,
    )


def place(ny, nz, nx):
    s, t = lax.axis_index("sp"), lax.axis_index("tp")
    z, y = s // ny, s % ny
    x, c = t // CORES, t % CORES

    def at(zz, yy, xx, cc):
        return (zz * ny + yy, xx * CORES + cc)

    return z, y, x, c, at


def layer_kernel(
    ny, nz, nx,
    q_lat, kv_lat, rope_key, cos_ref, sin_ref, q_gain, kv_gain, gain_ref, resid_ref,
    wqs_hbm, wql_hbm, wks_hbm, wkl_hbm, wos_hbm, wol_hbm, up_ref, dn_ref, out_ref,
    lat_out, up_out, dn_out, wqs, wql, wks, wkl, wos, wol, spread_ref, q_all,
    row_max, row_sum, weighted, part_ref, rs_c, rs_x, after, xg, hid,
    pbuf, cbuf, xbuf, zsend, zbuf, own_sem,
    lz_s, lz_r, ly_s, ly_r, lx_s, lx_r, lc_s, lc_r,
    uz_s, uz_r, uy_s, uy_r, dz_s, dz_r, dy_s, dy_r,
    ac_s, ac_r, ax_s, ax_r, bz_s, bz_r, bx_s, bx_r, bc_s, bc_r,
    cc_s, cc_r, cx_s, cx_r, cz_s, cz_r,
):
    z, y, x, c, at = place(ny, nz, nx)
    s = z * ny + y
    tp = nx * CORES
    t = x * CORES + c
    tok_rows = lat_out.shape[1]
    part = tok_rows // tp
    rank = kv_lat.shape[1]
    units = up_out.shape[2]
    rows, width = resid_ref.shape
    heads = q_all.shape[0]
    small = wks.shape[1] // (2 * SMALL_DIM)
    partner = at(z, y, x, 1 - c)
    zdev = [at((z + k) % nz, y, x, c) for k in range(nz)]
    zback = [at((z - k + nz) % nz, y, x, c) for k in range(nz)]
    ydev = [at(z, (y + j) % ny, x, c) for j in range(ny)]
    xdev = [at(z, y, (x + i) % nx, c) for i in range(nx)]
    zorder = near_first(nz)

    barrier = pltpu.get_barrier_semaphore()
    friends = zdev[1:] + ydev[1:] + xdev[1:] + [partner]
    for device in friends:
        pl.semaphore_signal(barrier, inc=1, device_id=device, device_id_type=MESH)

    def up_part(to):
        return up_ref.at[:, pl.ds(pl.multiple_of(to * units, LANES), units)]

    def dn_part(to):
        return dn_ref.at[pl.ds(pl.multiple_of(to * units, LANES), units), :]

    local = [
        pltpu.make_async_copy(src, dst, own_sem.at[i])
        for i, (src, dst) in enumerate(
            (
                (wqs_hbm, wqs),
                (wql_hbm, wql),
                (wks_hbm, wks),
                (wkl_hbm, wkl),
                (wos_hbm, wos),
                (wol_hbm, wol),
                (up_part(z), up_out.at[s]),
                (dn_part(z), dn_out.at[s]),
            )
        )
    ]
    for copy in local:
        copy.start()

    sent = []
    guard = [None]

    def start(make):
        sent.append((guard[-1], make))
        remote(*make()).start()

    def under(condition, body):
        guard.append(condition)
        pl.when(condition)(body)
        guard.pop()

    def arrive(make):
        remote(*make()).wait_recv()

    def zi(k):
        return (z - k + nz) % nz

    def block(k, j):
        return zi(k) * ny + (y - j + ny) % ny

    lane = lax.broadcasted_iota(jnp.int32, (tok_rows, LANES), 1)

    def turn(values):
        swapped = jnp.where(
            lane < HALF_ROPE,
            pltpu.roll(values, LANES - HALF_ROPE, 1),
            pltpu.roll(values, HALF_ROPE, 1),
        )
        turned = values * cos_ref[...] + swapped * sin_ref[...]
        return jnp.where(lane < ROPE_DIM, turned, 0.0)

    spread_ref[...] = jnp.zeros_like(spread_ref)
    spread_ref[:, :ROPE_DIM] = rope_key[...].astype(jnp.float32)
    lat_out[s, :, :rank] = rms_scale(kv_lat[...], kv_gain[...]).astype(jnp.bfloat16)
    lat_out[s, :, rank:] = turn(spread_ref[:, :LANES]).astype(jnp.bfloat16)

    with jax.named_scope("greet"):
        pl.semaphore_wait(barrier, len(friends))

    def share(b, p):
        return lat_out.at[b, pl.ds(pl.multiple_of(p * part, part), part)]

    def at_part(i, cc):
        return ((x - i + nx) % nx) * CORES + cc

    def lz(k, b):
        return lambda: (share(b(), t), share(b(), t), lz_s.at[k], lz_r.at[k], zdev[k])

    def ly(k, j, b):
        return lambda: (share(b(), t), share(b(), t), ly_s.at[k, j], ly_r.at[k, j], ydev[j])

    def lx(k, j, i, p):
        return lambda: (
            share(block(k, j), p()), share(block(k, j), p()),
            lx_s.at[k, j, i], lx_r.at[k, j, i], xdev[i],
        )

    def lc(k, j, i, cc):
        return lambda: (
            share(block(k, j), at_part(i, cc)), share(block(k, j), at_part(i, cc)),
            lc_s.at[k, j, i], lc_r.at[k, j, i], partner,
        )

    def lat_spread(k, j):
        for i in range(1, nx):
            start(lx(k, j, i, lambda: t))
        start(lc(k, j, 0, c))

    for k in zorder:
        under(z + k < nz, lambda k=k: start(lz(k, lambda: s)))
    for j in range(1, ny):
        under(y + j < ny, lambda j=j: start(ly(0, j, lambda: s)))

    def z_up(k):
        return lambda: (up_part((z + k) % nz), up_out.at[s], uz_s.at[k], uz_r.at[k], zdev[k])

    def z_dn(k):
        return lambda: (dn_part((z + k) % nz), dn_out.at[s], dz_s.at[k], dz_r.at[k], zdev[k])

    for k in zorder:
        start(z_up(k))
    for k in zorder:
        start(z_dn(k))
    for j in range(1, ny):
        start(lambda j=j: (up_part(z), up_out.at[s], uy_s.at[0, j], uy_r.at[0, j], ydev[j]))

    def up_forward(k):
        slot = lambda: up_out.at[block(k, 0)]
        arrive(lambda: (slot(), slot(), uz_s.at[k], uz_r.at[k], zdev[k]))
        for j in range(1, ny):
            start(lambda j=j: (slot(), slot(), uy_s.at[k, j], uy_r.at[k, j], ydev[j]))

    def dn_forward(k):
        slot = lambda: dn_out.at[block(k, 0)]
        arrive(lambda: (slot(), slot(), dz_s.at[k], dz_r.at[k], zdev[k]))
        for j in range(1, ny):
            start(lambda j=j: (slot(), slot(), dy_s.at[k, j], dy_r.at[k, j], ydev[j]))

    with jax.named_scope("queries"):
        query_normed = rms_scale(q_lat[...], q_gain[...]).astype(jnp.bfloat16)
        head = 0
        for w_ref, copies, nope in ((wqs, local[0], SMALL_DIM), (wql, local[1], LARGE_DIM)):
            copies.wait()
            cols = w_ref.shape[1]
            spread_ref[:, :cols] = jnp.dot(
                query_normed, w_ref[...], preferred_element_type=jnp.float32
            )

            def take(first, size):
                b, off = first // LANES, first % LANES
                got = spread_ref[:, b * LANES : (b + 1) * LANES]
                if off:
                    got = pltpu.roll(got, LANES - off, 1)
                if off + size > LANES:
                    more = spread_ref[:, (b + 1) * LANES : (b + 2) * LANES]
                    got = jnp.where(lane < LANES - off, got, pltpu.roll(more, LANES - off, 1))
                return got

            for h in range(cols // (nope + ROPE_DIM)):
                first = h * (nope + ROPE_DIM)
                content = take(first, nope)
                if nope < LANES:
                    content = jnp.where(lane < nope, content, 0.0)
                q_all[head, :, :LANES] = content.astype(jnp.bfloat16)
                q_all[head, :, LANES:] = turn(take(first + nope, ROPE_DIM)).astype(jnp.bfloat16)
                head += 1
    local[2].wait()
    local[3].wait()

    def attend(latents, causal, first):
        latent = latents[:, :rank]
        turned = latents[:, rank:]
        kv_small = jnp.dot(latent, wks[...], preferred_element_type=jnp.float32)
        kv_small = kv_small.astype(jnp.bfloat16)
        kv_large = jnp.dot(latent, wkl[...], preferred_element_type=jnp.float32)
        kv_large = kv_large.astype(jnp.bfloat16)
        for h in range(heads):
            if h < small:
                key = kv_small[:, 2 * SMALL_DIM * h : 2 * SMALL_DIM * (h + 1)]
                value = key
                scale = (SMALL_DIM + ROPE_DIM) ** (-0.5)
            else:
                begin = 2 * LARGE_DIM * (h - small)
                key = kv_large[:, begin : begin + LARGE_DIM]
                value = kv_large[:, begin + LARGE_DIM : begin + 2 * LARGE_DIM]
                scale = (LARGE_DIM + ROPE_DIM) ** (-0.5)
            scores = lax.dot_general(
                q_all[h],
                jnp.concatenate([key, turned], axis=1),
                (((1,), (1,)), ((), ())),
                preferred_element_type=jnp.float32,
            )
            scores = scores * (scale * LOG2E)
            if causal is not None:
                scores = jnp.where(causal, scores, -1e30)
            top = jnp.max(scores, axis=-1, keepdims=True)
            if first:
                weights = jnp.exp2(scores - top)
                row_max[h] = top
                row_sum[h] = jnp.sum(weights, axis=-1, keepdims=True)
                weighted[h] = jnp.dot(
                    weights.astype(jnp.bfloat16), value, preferred_element_type=jnp.float32
                )
                continue
            old_max = row_max[h]
            new_max = jnp.maximum(old_max, top)
            shrink = jnp.exp2(old_max - new_max)
            weights = jnp.exp2(scores - new_max)
            row_max[h] = new_max
            row_sum[h] = row_sum[h] * shrink + jnp.sum(weights, axis=-1, keepdims=True)
            weighted[h] = weighted[h] * shrink + jnp.dot(
                weights.astype(jnp.bfloat16), value, preferred_element_type=jnp.float32
            )

    def lat_from_z(k):
        slot = lambda: block(k, 0)
        arrive(lz(k, slot))
        for j in range(1, ny):
            start(ly(k, j, slot))
        lat_spread(k, 0)

    def lat_from_y(k, j):
        arrive(ly(k, j, lambda: block(k, j)))
        lat_spread(k, j)

    def lat_from_x(k, j):
        for i in range(1, nx):
            arrive(lx(k, j, i, lambda i=i: at_part(i, c)))
            start(lc(k, j, i, c))

    def lat_here(k, j):
        for i in range(nx):
            arrive(lc(k, j, i, 1 - c))

    with jax.named_scope("own"):
        ahead = lax.broadcasted_iota(jnp.int32, (tok_rows, tok_rows), 1) <= (
            lax.broadcasted_iota(jnp.int32, (tok_rows, tok_rows), 0)
        )
        attend(lat_out[s], ahead, True)
    with jax.named_scope("lat_z"):
        for k in zorder:
            under(z >= k, lambda k=k: lat_from_z(k))
        for j in range(1, ny):
            under(y >= j, lambda j=j: lat_from_y(0, j))
    for j in range(1, ny):
        start(lambda j=j: (dn_part(z), dn_out.at[s], dy_s.at[0, j], dy_r.at[0, j], ydev[j]))
    with jax.named_scope("lat_x0"):
        for j in range(1, ny):
            under(y >= j, lambda j=j: lat_from_x(0, j))
        for k in zorder:
            under(z >= k, lambda k=k: lat_from_x(k, 0))
        for j in range(1, ny):
            under(y >= j, lambda j=j: lat_here(0, j))
    with jax.named_scope("near"):
        def near(j, carry):
            attend(lat_out[z * ny + j], None, False)
            return carry

        lax.fori_loop(0, y, near, 0)
    with jax.named_scope("lat_y"):
        for k in zorder:
            for j in range(1, ny):
                under(z >= k, lambda k=k, j=j: lat_from_y(k, j))
        for k in zorder:
            for j in range(1, ny):
                under(z >= k, lambda k=k, j=j: lat_from_x(k, j))
    with jax.named_scope("up_fwd"):
        for k in zorder[:2]:
            up_forward(k)
    with jax.named_scope("lat_all"):
        for k in zorder:
            for j in range(ny):
                under(z >= k, lambda k=k, j=j: lat_here(k, j))
    with jax.named_scope("far"):
        def far(zz, carry):
            latents = lat_out[pl.ds(zz * ny, ny)].reshape(ny * tok_rows, lat_out.shape[2])
            attend(latents, None, False)
            return carry

        lax.fori_loop(0, z, far, 0)
    local[4].wait()
    local[5].wait()
    with jax.named_scope("outproj"):
        parts = []
        for h in range(heads):
            head_out = (weighted[h] / row_sum[h]).astype(jnp.bfloat16)
            parts.append(head_out[:, SMALL_DIM:] if h < small else head_out)
        from_small = jnp.concatenate(parts[:small], axis=1)
        from_large = jnp.concatenate(parts[small:], axis=1)
        cut = width // HALVES

        def ac(i):
            return lambda: (part_ref.at[i, 1 - c], rs_c.at[i], ac_s.at[i], ac_r.at[i], partner)

        def ax(i, j):
            return lambda: (
                part_ref.at[i, c, (x + j) % nx], rs_x.at[i, j], ax_s.at[i, j], ax_r.at[i, j], xdev[j]
            )

        for i in range(HALVES):
            mixed = jnp.dot(
                from_small, wos[:, i * cut : (i + 1) * cut], preferred_element_type=jnp.float32
            ) + jnp.dot(
                from_large, wol[:, i * cut : (i + 1) * cut], preferred_element_type=jnp.float32
            )
            mixed = mixed.astype(jnp.bfloat16)
            for xx in range(nx):
                for cc in range(CORES):
                    first = (xx * CORES + cc) * rows
                    part_ref[i, cc, xx] = mixed[first : first + rows]
            start(ac(i))
    with jax.named_scope("rs_core"):
        for i in range(HALVES):
            arrive(ac(i))
            part_ref[i, c] = (
                part_ref[i, c].astype(jnp.float32) + rs_c[i].astype(jnp.float32)
            ).astype(jnp.bfloat16)
            for j in range(1, nx):
                start(ax(i, j))
    with jax.named_scope("fwd2"):
        for k in zorder[2:]:
            up_forward(k)
        for k in zorder[:2]:
            dn_forward(k)
    with jax.named_scope("rs_x"):
        for i in range(HALVES):
            mixed = part_ref[i, c, x].astype(jnp.float32)
            for j in range(1, nx):
                arrive(ax(i, j))
                mixed = mixed + rs_x[i, j].astype(jnp.float32)
            piece = resid_ref[:, i * cut : (i + 1) * cut].astype(jnp.float32) + mixed
            after[:, i * cut : (i + 1) * cut] = piece.astype(jnp.bfloat16)
        xg[z, c, x] = rms_scale(after[...], gain_ref[...]).astype(jnp.bfloat16)

    def bz(k):
        slot = lambda: xg.at[z, c, x]
        return lambda: (slot(), slot(), bz_s.at[k], bz_r.at[z], zdev[k])

    def spread(a):
        slot = lambda: xg.at[a, c, x]
        for i in range(1, nx):
            start(lambda i=i: (slot(), slot(), bx_s.at[a, i], bx_r.at[a, i], xdev[i]))
        start(lambda: (slot(), slot(), bc_s.at[a, 0], bc_r.at[a, 0], partner))

    for k in zorder:
        start(bz(k))
    spread(z)
    with jax.named_scope("fwd3"):
        for k in zorder[2:]:
            dn_forward(k)
    with jax.named_scope("g_z"):
        for a in range(nz):
            def from_z(a=a):
                slot = lambda: xg.at[a, c, x]
                arrive(lambda: (slot(), slot(), bz_s.at[0], bz_r.at[a], partner))
                for i in range(1, nx):
                    start(lambda i=i: (slot(), slot(), bx_s.at[a, i], bx_r.at[a, i], xdev[i]))
                start(lambda: (slot(), slot(), bc_s.at[a, 0], bc_r.at[a, 0], partner))

            under(z != a, from_z)

    def xi(i):
        return (x - i + nx) % nx

    def from_x(a):
        for i in range(1, nx):
            slot = lambda i=i: xg.at[a, c, xi(i)]
            arrive(lambda: (slot(), slot(), bx_s.at[a, i], bx_r.at[a, i], xdev[i]))
            start(lambda i=i, slot=slot: (slot(), slot(), bc_s.at[a, i], bc_r.at[a, i], partner))

    def rows_here(a):
        for i in range(nx):
            slot = lambda i=i: xg.at[a, 1 - c, xi(i)]
            arrive(lambda: (slot(), slot(), bc_s.at[a, i], bc_r.at[a, i], partner))

    def weights_here(out, sy, ry):
        for k in range(nz):
            for j in range(1, ny):
                slot = lambda: out.at[block(k, j)]
                arrive(lambda: (slot(), slot(), sy.at[k, j], ry.at[k, j], ydev[j]))

    def up_step(a):
        rows_here(a)
        tokens = xg[a].reshape(tp * rows, width)
        projected = jnp.dot(
            tokens, up_out[...].reshape(width, units), preferred_element_type=jnp.float32
        )
        hid[a] = jnp.square(jnp.maximum(projected, 0.0)).astype(jnp.bfloat16)

    def down_step(k):
        hidden = hid[zi(k)]
        cols = dn_out.shape[2]
        for b in range(dn_out.shape[0]):
            out = jnp.dot(hidden, dn_out[b], preferred_element_type=jnp.float32)
            pbuf[k, :, :, :, b * cols : (b + 1) * cols] = out.astype(jnp.bfloat16).reshape(
                CORES, nx, rows, cols
            )
        start(lambda: (pbuf.at[k, 1 - c], cbuf.at[k], cc_s.at[k], cc_r.at[k], partner))

    def core_sum(k):
        arrive(lambda: (cbuf.at[k], cbuf.at[k], cc_s.at[k], cc_r.at[k], partner))
        pbuf[k, c] = (
            pbuf[k, c].astype(jnp.float32) + cbuf[k].astype(jnp.float32)
        ).astype(jnp.bfloat16)
        for j in range(1, nx):
            start(
                lambda j=j: (
                    pbuf.at[k, c, (x + j) % nx], xbuf.at[k, j], cx_s.at[k, j], cx_r.at[k, j], xdev[j]
                )
            )

    def cross_sum(k):
        summed = pbuf[k, c, x].astype(jnp.float32)
        for j in range(1, nx):
            arrive(lambda: (xbuf.at[k, j], xbuf.at[k, j], cx_s.at[k, j], cx_r.at[k, j], xdev[j]))
            summed = summed + xbuf[k, j].astype(jnp.float32)
        zsend[k] = summed.astype(jnp.bfloat16)
        if k:
            start(lambda: (zsend.at[k], zbuf.at[k], cz_s.at[k], cz_r.at[k], zback[k]))

    with jax.named_scope("g_x"):
        from_x(0)
    local[6].wait()
    with jax.named_scope("w_up"):
        weights_here(up_out, uy_s, uy_r)
    for a in range(nz):
        if a + 1 < nz:
            with jax.named_scope("g_x"):
                from_x(a + 1)
        with jax.named_scope("up"):
            up_step(a)
    local[7].wait()
    with jax.named_scope("w_dn"):
        weights_here(dn_out, dy_s, dy_r)
    order = zorder[::-1] + [0]
    with jax.named_scope("down"):
        for i, k in enumerate(order):
            down_step(k)
            if i:
                core_sum(order[i - 1])
        core_sum(order[-1])
    for k in order:
        with jax.named_scope("cross"):
            cross_sum(k)
    with jax.named_scope("final"):
        final = after[...].astype(jnp.float32)
        ffn = zsend[0].astype(jnp.float32)
        for k in order[:-1]:
            arrive(lambda: (zbuf.at[k], zbuf.at[k], cz_s.at[k], cz_r.at[k], zback[k]))
            ffn = ffn + zbuf[k].astype(jnp.float32)
        out_ref[...] = (final + ffn).astype(jnp.bfloat16)

    def finish(make):
        remote(*make()).wait_send()

    with jax.named_scope("wait_send"):
        for condition, make in sent:
            if condition is None:
                finish(make)
            else:
                pl.when(condition)(functools.partial(finish, make))


def layer(
    ny, nz, nx, q_lat, kv_lat, rope_key, cos, sin, q_gain, kv_gain, gain, resid,
    wqs, wql, wks, wkl, wos, wol, w_up, w_down,
):
    tp, sp = nx * CORES, ny * nz
    rows, width = resid.shape
    tok_rows, rank = kv_lat.shape
    small = wks.shape[1] // (2 * SMALL_DIM)
    large = wkl.shape[1] // (2 * LARGE_DIM)
    heads = small + large
    units = w_up.shape[1] // nz
    query_cols = -(-max(wqs.shape[1], wql.shape[1]) // LANES) * LANES
    dma = pltpu.SemaphoreType.DMA
    vmem = pl.BlockSpec(memory_space=pltpu.VMEM)
    anywhere = pl.BlockSpec(memory_space=pl.ANY)
    b16, f32 = jnp.bfloat16, jnp.float32

    def pair(*shape):
        return [dma(shape), dma(shape)]

    def like(array):
        return pltpu.VMEM(array.shape, array.dtype)

    return pl.pallas_call(
        functools.partial(layer_kernel, ny, nz, nx),
        out_shape=jax.ShapeDtypeStruct((rows, width), b16),
        in_specs=[vmem] * 9 + [anywhere] * 8,
        out_specs=vmem,
        scratch_shapes=[
            pltpu.VMEM((sp, tok_rows, rank + LANES), b16),
            pltpu.VMEM((sp, w_up.shape[0], units), b16),
            pltpu.VMEM((sp, units, w_down.shape[1]), b16),
            like(wqs),
            like(wql),
            like(wks),
            like(wkl),
            like(wos),
            like(wol),
            pltpu.VMEM((tok_rows, query_cols), f32),
            pltpu.VMEM((heads, tok_rows, 2 * LANES), b16),
            pltpu.VMEM((heads, tok_rows, 1), f32),
            pltpu.VMEM((heads, tok_rows, 1), f32),
            pltpu.VMEM((heads, tok_rows, LARGE_DIM), f32),
            pltpu.VMEM((HALVES, CORES, nx, rows, width // HALVES), b16),
            pltpu.VMEM((HALVES, nx, rows, width // HALVES), b16),
            pltpu.VMEM((HALVES, nx, rows, width // HALVES), b16),
            pltpu.VMEM((rows, width), b16),
            pltpu.VMEM((nz, CORES, nx, rows, width), b16),
            pltpu.VMEM((nz, tp * rows, units), b16),
            pltpu.VMEM((nz, CORES, nx, rows, width), b16),
            pltpu.VMEM((nz, nx, rows, width), b16),
            pltpu.VMEM((nz, nx, rows, width), b16),
            pltpu.VMEM((nz, rows, width), b16),
            pltpu.VMEM((nz, rows, width), b16),
            dma((8,)),
        ]
        + pair(nz)
        + pair(nz, ny)
        + pair(nz, ny, nx) * 2
        + (pair(nz) + pair(nz, ny)) * 2
        + pair(HALVES)
        + pair(HALVES, nx)
        + pair(nz)
        + pair(nz, nx) * 2
        + pair(nz)
        + pair(nz, nx)
        + pair(nz),
        compiler_params=pltpu.CompilerParams(
            collective_id=1, has_side_effects=True, vmem_limit_bytes=63 * 2**20
        ),
        name="layer",
    )(
        q_lat, kv_lat, rope_key, cos, sin, q_gain, kv_gain, gain, resid,
        wqs, wql, wks, wkl, wos, wol, w_up, w_down,
    )


def on_device(
    ny,
    nz,
    nx,
    resid,
    q_latent,
    kv_latent,
    rope_key,
    q_gain,
    kv_gain,
    w_q_small,
    w_q_large,
    w_kv_small,
    w_kv_large,
    w_out_small,
    w_out_large,
    ffn_gain,
    w_up,
    w_down,
):
    tok_rows = q_latent.shape[0]
    offset = lax.axis_index("sp") * tok_rows
    cos, sin = rotary_tables(offset + jnp.arange(tok_rows, dtype=jnp.int32))
    return layer(
        ny,
        nz,
        nx,
        q_latent,
        kv_latent,
        rope_key,
        cos,
        sin,
        q_gain.reshape(1, -1),
        kv_gain.reshape(1, -1),
        ffn_gain.reshape(1, -1),
        resid,
        w_q_small,
        w_q_large,
        w_kv_small,
        w_kv_large,
        w_out_small,
        w_out_large,
        w_up,
        w_down,
    )


def solution(mesh):
    ny = inner_split(mesh.shape["sp"])
    nz = mesh.shape["sp"] // ny
    nx = mesh.shape["tp"] // CORES
    return jax.shard_map(
        functools.partial(on_device, ny, nz, nx),
        mesh=mesh,
        in_specs=(
            P(("sp", "tp"), None),
            P("sp", None),
            P("sp", None),
            P("sp", None),
            P(),
            P(),
            P(None, "tp"),
            P(None, "tp"),
            P(None, "tp"),
            P(None, "tp"),
            P("tp", None),
            P("tp", None),
            P(),
            P("sp", "tp"),
            P("tp", "sp"),
        ),
        out_specs=P(("sp", "tp"), None),
        check_vma=False,
    )
```

```python
import functools

import jax
import jax.numpy as jnp
from jax import lax
from jax.experimental import pallas as pl
from jax.experimental.pallas import tpu as pltpu
from jax.sharding import PartitionSpec as P

SMALL_DIM = 64
LARGE_DIM = 128
ROPE_DIM = 32
HALF_ROPE = ROPE_DIM // 2

epsilon = 1e-06
theta_base = 10000.0
LOG2E = 1.4426950408889634

MESH = pl.DeviceIdType.MESH
CORES = 2
LANES = 128
HALVES = 2


def rms_scale(inputs, gain_vec):
    values = inputs.astype(jnp.float32)
    return (
        values * lax.rsqrt(jnp.mean(values * values, axis=-1, keepdims=True) + epsilon) * gain_vec
    )


def rotary_tables(positions):
    exponent = jnp.arange(0, ROPE_DIM, 2, dtype=jnp.float32) / ROPE_DIM
    angles = (theta_base ** (-exponent))[:, None] * positions.astype(jnp.float32)[None, :]
    return jnp.cos(angles), jnp.sin(angles)


def inner_split(count):
    best = 1
    for size in range(1, count + 1):
        if size * size <= count and count % size == 0:
            best = size
    return best


def outward(count, z, i):
    orders = [
        sorted(range(count), key=lambda a: (abs(a - zz), a if 2 * zz < count else -a))
        for zz in range(count)
    ]
    got = orders[0][i]
    for zz in range(1, count):
        got = got + jnp.minimum(jnp.maximum(z - (zz - 1), 0), 1) * (orders[zz][i] - orders[zz - 1][i])
    return got


def remote(src, dst, send_sem, recv_sem, device):
    return pltpu.make_async_remote_copy(
        src_ref=src,
        dst_ref=dst,
        send_sem=send_sem,
        recv_sem=recv_sem,
        device_id=device,
        device_id_type=MESH,
    )


def place(ny, nz, nx):
    s, t = lax.axis_index("sp"), lax.axis_index("tp")
    z, y = s // ny, s % ny
    x, c = t // CORES, t % CORES

    def at(zz, yy, xx, cc):
        return (zz * ny + yy, xx * CORES + cc)

    return z, y, x, c, at


def layer_kernel(
    ny, nz, nx,
    q_lat, kv_lat, rope_t, cos_t, sin_t, q_gain, kv_gain, gain_ref, resid_ref,
    wqs_hbm, wql_hbm, wks_hbm, wkl_hbm, wos_hbm, wol_hbm, up_ref, dn_ref, out_ref,
    lat_out, up_out, dn_out, wqs, wql, wks, wkl, wos, wol, stood, spread_ref, q_all,
    row_max, row_sum, weighted, part_ref, rs_c, rs_x, after, xg, hid,
    pbuf, cbuf, xbuf, zsend, zbuf, own_sem, go_sem,
    lz_s, lz_r, ly_s, ly_r, lx_s, lx_r, lc_s, lc_r,
    uz_s, uz_r, uy_s, uy_r, dz_s, dz_r, dy_s, dy_r,
    ac_s, ac_r, ax_s, ax_r, bz_s, bz_r, bo_s, bx_s, bx_r, bc_s, bc_r,
    cc_s, cc_r, cx_s, cx_r, cz_s, cz_r,
):
    z, y, x, c, at = place(ny, nz, nx)
    s = z * ny + y
    tp = nx * CORES
    t = x * CORES + c
    tok_rows = lat_out.shape[1]
    part = tok_rows // tp
    rank = kv_lat.shape[1]
    units = up_out.shape[2]
    rows, width = resid_ref.shape
    heads = q_all.shape[0]
    small = wks.shape[1] // (2 * SMALL_DIM)
    partner = at(z, y, x, 1 - c)
    zdev = [at((z + k) % nz, y, x, c) for k in range(nz)]
    ydev = [at(z, (y + j) % ny, x, c) for j in range(ny)]
    xdev = [at(z, y, (x + i) % nx, c) for i in range(nx)]
    turns = [outward(nz, z, i) for i in range(nz)]
    zabs = [at(a, y, x, c) for a in turns]
    far_first = list(range(nz - 1, 0, -1))

    barrier = pltpu.get_barrier_semaphore()
    friends = zdev[1:] + ydev[1:] + xdev[1:] + [partner]
    for device in friends:
        pl.semaphore_signal(barrier, inc=1, device_id=device, device_id_type=MESH)

    def up_part(to):
        return up_ref.at[:, pl.ds(pl.multiple_of(to * units, LANES), units)]

    def dn_part(to):
        first = to * units
        if not isinstance(first, int):
            first = pl.multiple_of(first, LANES)
        return dn_ref.at[pl.ds(first, units), :]

    local = [
        pltpu.make_async_copy(src, dst, own_sem.at[i])
        for i, (src, dst) in enumerate(
            (
                (wqs_hbm, wqs),
                (wql_hbm, wql),
                (wks_hbm, wks),
                (wkl_hbm, wkl),
                (wos_hbm, wos),
                (wol_hbm, wol),
                (up_part(z), up_out.at[s]),
                (dn_part(z), dn_out.at[s]),
            )
        )
    ]
    for copy in local:
        copy.start()

    sent = []
    guard = [None]

    def finish(make):
        remote(*make()).wait_send()

    def drain():
        for condition, make in sent:
            if condition is None:
                finish(make)
            else:
                pl.when(condition)(functools.partial(finish, make))
        sent.clear()

    def start(make):
        sent.append((guard[-1], make))
        remote(*make()).start()

    def under(condition, body):
        guard.append(condition)
        pl.when(condition)(body)
        guard.pop()

    def arrive(make):
        remote(*make()).wait_recv()

    def zi(k):
        return (z - k + nz) % nz

    def block(k, j):
        return zi(k) * ny + (y - j + ny) % ny

    lane = lax.broadcasted_iota(jnp.int32, (tok_rows, LANES), 1)

    low = rope_t[:HALF_ROPE].astype(jnp.float32)
    high = rope_t[HALF_ROPE:].astype(jnp.float32)
    cos, sin = cos_t[...], sin_t[...]
    stood[...] = jnp.zeros_like(stood)
    stood[:HALF_ROPE] = low * cos - high * sin
    stood[HALF_ROPE:ROPE_DIM] = high * cos + low * sin
    lat_out[s, :, rank:] = stood[...].T.astype(jnp.bfloat16)
    lat_out[s, :, :rank] = rms_scale(kv_lat[...], kv_gain[...]).astype(jnp.bfloat16)

    with jax.named_scope("greet"):
        pl.semaphore_wait(barrier, len(friends))

    def share(b, p):
        return lat_out.at[b, pl.ds(pl.multiple_of(p * part, part), part)]

    def at_part(i, cc):
        return ((x - i + nx) % nx) * CORES + cc

    def lz(k, b):
        return lambda: (share(b(), t), share(b(), t), lz_s.at[k], lz_r.at[k], zdev[k])

    def ly(k, j, b):
        return lambda: (share(b(), t), share(b(), t), ly_s.at[k, j], ly_r.at[k, j], ydev[j])

    def lx(k, j, i, p):
        return lambda: (
            share(block(k, j), p()), share(block(k, j), p()),
            lx_s.at[k, j, i], lx_r.at[k, j, i], xdev[i],
        )

    def lc(k, j, i, cc):
        return lambda: (
            share(block(k, j), at_part(i, cc)), share(block(k, j), at_part(i, cc)),
            lc_s.at[k, j, i], lc_r.at[k, j, i], partner,
        )

    def lat_spread(k, j):
        for i in range(1, nx):
            start(lx(k, j, i, lambda: t))
        start(lc(k, j, 0, c))

    for k in range(1, nz):
        under(z + k < nz, lambda k=k: start(lz(k, lambda: s)))
    for j in range(1, ny):
        under(y + j < ny, lambda j=j: start(ly(0, j, lambda: s)))

    def z_up(i):
        a = turns[i]
        return lambda: (up_part(a), up_out.at[s], uz_s.at[i], uz_r.at[z], zabs[i])

    def z_dn(i):
        a = turns[i]
        return lambda: (dn_part(a), dn_out.at[s], dz_s.at[i], dz_r.at[z], zabs[i])

    def forward(i, out, zs, zr, ys, yr):
        a = turns[i]
        slot = lambda: out.at[a * ny + y]
        arrive(lambda: (slot(), slot(), zs.at[i], zr.at[a], zabs[i]))
        for j in range(1, ny):
            start(lambda j=j: (slot(), slot(), ys.at[a, j], yr.at[a, j], ydev[j]))

    def up_forward(i):
        forward(i, up_out, uz_s, uz_r, uy_s, uy_r)

    def dn_forward(i):
        forward(i, dn_out, dz_s, dz_r, dy_s, dy_r)

    with jax.named_scope("queries"):
        stood[:HALF_ROPE] = cos
        stood[HALF_ROPE:ROPE_DIM] = cos
        cos_ref = stood[...].T
        stood[:HALF_ROPE] = -sin
        stood[HALF_ROPE:ROPE_DIM] = sin
        sin_ref = stood[...].T

        def turn(values):
            swapped = jnp.where(
                lane < HALF_ROPE,
                pltpu.roll(values, LANES - HALF_ROPE, 1),
                pltpu.roll(values, HALF_ROPE, 1),
            )
            turned = values * cos_ref + swapped * sin_ref
            return jnp.where(lane < ROPE_DIM, turned, 0.0)

        spread_ref[...] = jnp.zeros_like(spread_ref)
        values = q_lat[...].astype(jnp.float32)
        values = values * lax.rsqrt(jnp.mean(values * values, axis=-1, keepdims=True) + epsilon)
        query_normed = jnp.concatenate(
            [
                values[:, b * LANES : (b + 1) * LANES] * q_gain[b : b + 1]
                for b in range(values.shape[1] // LANES)
            ],
            axis=1,
        ).astype(jnp.bfloat16)
        head = 0
        for w_ref, copies, nope in ((wqs, local[0], SMALL_DIM), (wql, local[1], LARGE_DIM)):
            copies.wait()
            cols = w_ref.shape[0]
            spread_ref[:, :cols] = lax.dot_general(
                query_normed,
                w_ref[...],
                (((1,), (1,)), ((), ())),
                preferred_element_type=jnp.float32,
            )

            def take(first, size):
                b, off = first // LANES, first % LANES
                got = spread_ref[:, b * LANES : (b + 1) * LANES]
                if off:
                    got = pltpu.roll(got, LANES - off, 1)
                if off + size > LANES:
                    more = spread_ref[:, (b + 1) * LANES : (b + 2) * LANES]
                    got = jnp.where(lane < LANES - off, got, pltpu.roll(more, LANES - off, 1))
                return got

            for h in range(cols // (nope + ROPE_DIM)):
                first = h * (nope + ROPE_DIM)
                content = take(first, nope)
                if nope < LANES:
                    content = jnp.where(lane < nope, content, 0.0)
                q_all[head, :, :LANES] = content.astype(jnp.bfloat16)
                q_all[head, :, LANES:] = turn(take(first + nope, ROPE_DIM)).astype(jnp.bfloat16)
                head += 1
    local[2].wait()
    local[3].wait()

    def attend(latents, causal, first):
        latent = latents[:, :rank]
        turned = latents[:, rank:]
        kv_small = jnp.dot(latent, wks[...], preferred_element_type=jnp.float32)
        kv_small = kv_small.astype(jnp.bfloat16)
        kv_large = jnp.dot(latent, wkl[...], preferred_element_type=jnp.float32)
        kv_large = kv_large.astype(jnp.bfloat16)
        for h in range(heads):
            if h < small:
                key = kv_small[:, 2 * SMALL_DIM * h : 2 * SMALL_DIM * (h + 1)]
                value = key
                scale = (SMALL_DIM + ROPE_DIM) ** (-0.5)
            else:
                begin = 2 * LARGE_DIM * (h - small)
                key = kv_large[:, begin : begin + LARGE_DIM]
                value = kv_large[:, begin + LARGE_DIM : begin + 2 * LARGE_DIM]
                scale = (LARGE_DIM + ROPE_DIM) ** (-0.5)
            scores = lax.dot_general(
                q_all[h],
                jnp.concatenate([key, turned], axis=1),
                (((1,), (1,)), ((), ())),
                preferred_element_type=jnp.float32,
            )
            scores = scores * (scale * LOG2E)
            if causal is not None:
                scores = jnp.where(causal, scores, -1e30)
            top = jnp.max(scores, axis=-1, keepdims=True)
            if first:
                weights = jnp.exp2(scores - top)
                row_max[h] = top
                row_sum[h] = jnp.sum(weights, axis=-1, keepdims=True)
                weighted[h] = jnp.dot(
                    weights.astype(jnp.bfloat16), value, preferred_element_type=jnp.float32
                )
                continue
            old_max = row_max[h]
            new_max = jnp.maximum(old_max, top)
            shrink = jnp.exp2(old_max - new_max)
            weights = jnp.exp2(scores - new_max)
            row_max[h] = new_max
            row_sum[h] = row_sum[h] * shrink + jnp.sum(weights, axis=-1, keepdims=True)
            weighted[h] = weighted[h] * shrink + jnp.dot(
                weights.astype(jnp.bfloat16), value, preferred_element_type=jnp.float32
            )

    def lat_from_z(k):
        slot = lambda: block(k, 0)
        arrive(lz(k, slot))
        for j in range(1, ny):
            start(ly(k, j, slot))
        lat_spread(k, 0)

    def lat_from_y(k, j):
        arrive(ly(k, j, lambda: block(k, j)))
        lat_spread(k, j)

    def lat_from_x(k, j):
        for i in range(1, nx):
            arrive(lx(k, j, i, lambda i=i: at_part(i, c)))
            start(lc(k, j, i, c))

    def lat_here(k, j):
        for i in range(nx):
            arrive(lc(k, j, i, 1 - c))

    with jax.named_scope("own"):
        ahead = lax.broadcasted_iota(jnp.int32, (tok_rows, tok_rows), 1) <= (
            lax.broadcasted_iota(jnp.int32, (tok_rows, tok_rows), 0)
        )
        attend(lat_out[s], ahead, True)
    with jax.named_scope("drain"):
        drain()
        pl.semaphore_signal(go_sem, inc=1, device_id=partner, device_id_type=MESH)
        pl.semaphore_wait(go_sem, 1)
    for i in far_first:
        start(z_up(i))
    for i in far_first:
        start(z_dn(i))
    for j in range(1, ny):
        start(lambda j=j: (up_part(z), up_out.at[s], uy_s.at[z, j], uy_r.at[z, j], ydev[j]))
    with jax.named_scope("lat_z"):
        for k in range(1, nz):
            under(z >= k, lambda k=k: lat_from_z(k))
        for j in range(1, ny):
            under(y >= j, lambda j=j: lat_from_y(0, j))
    with jax.named_scope("lat_x0"):
        for j in range(1, ny):
            under(y >= j, lambda j=j: lat_from_x(0, j))
        for k in range(1, nz):
            under(z >= k, lambda k=k: lat_from_x(k, 0))
    with jax.named_scope("lat_c0"):
        for j in range(1, ny):
            under(y >= j, lambda j=j: lat_here(0, j))
    with jax.named_scope("near"):
        def near(j, carry):
            attend(lat_out[z * ny + j], None, False)
            return carry

        lax.fori_loop(0, y, near, 0)
    with jax.named_scope("lat_y"):
        for k in range(1, nz):
            for j in range(1, ny):
                under(z >= k, lambda k=k, j=j: lat_from_y(k, j))
        for k in range(1, nz):
            for j in range(1, ny):
                under(z >= k, lambda k=k, j=j: lat_from_x(k, j))
    for j in range(1, ny):
        start(lambda j=j: (dn_part(z), dn_out.at[s], dy_s.at[z, j], dy_r.at[z, j], ydev[j]))
    with jax.named_scope("up_fwd"):
        for i in far_first[:1]:
            up_forward(i)
    with jax.named_scope("lat_all"):
        for k in range(1, nz):
            for j in range(ny):
                under(z >= k, lambda k=k, j=j: lat_here(k, j))
    with jax.named_scope("far"):
        def far(zz, carry):
            latents = lat_out[pl.ds(zz * ny, ny)].reshape(ny * tok_rows, lat_out.shape[2])
            attend(latents, None, False)
            return carry

        lax.fori_loop(0, z, far, 0)
    local[4].wait()
    local[5].wait()
    with jax.named_scope("outproj"):
        parts = []
        for h in range(heads):
            head_out = (weighted[h] / row_sum[h]).astype(jnp.bfloat16)
            parts.append(head_out[:, SMALL_DIM:] if h < small else head_out)
        from_small = jnp.concatenate(parts[:small], axis=1)
        from_large = jnp.concatenate(parts[small:], axis=1)
        cut = width // HALVES

        def ac(i):
            return lambda: (part_ref.at[i, 1 - c], rs_c.at[i], ac_s.at[i], ac_r.at[i], partner)

        def ax(i, j):
            return lambda: (
                part_ref.at[i, c, (x + j) % nx], rs_x.at[i, j], ax_s.at[i, j], ax_r.at[i, j], xdev[j]
            )

        for i in range(HALVES):
            mixed = jnp.dot(
                from_small, wos[:, i * cut : (i + 1) * cut], preferred_element_type=jnp.float32
            ) + jnp.dot(
                from_large, wol[:, i * cut : (i + 1) * cut], preferred_element_type=jnp.float32
            )
            mixed = mixed.astype(jnp.bfloat16)
            for xx in range(nx):
                for cc in range(CORES):
                    first = (xx * CORES + cc) * rows
                    part_ref[i, cc, xx] = mixed[first : first + rows]
            start(ac(i))
    with jax.named_scope("rs_core"):
        for i in range(HALVES):
            arrive(ac(i))
            part_ref[i, c] = (
                part_ref[i, c].astype(jnp.float32) + rs_c[i].astype(jnp.float32)
            ).astype(jnp.bfloat16)
            for j in range(1, nx):
                start(ax(i, j))
    with jax.named_scope("fwd2"):
        for i in far_first[1:]:
            up_forward(i)
    with jax.named_scope("rs_x"):
        for i in range(HALVES):
            mixed = part_ref[i, c, x].astype(jnp.float32)
            for j in range(1, nx):
                arrive(ax(i, j))
                mixed = mixed + rs_x[i, j].astype(jnp.float32)
            piece = resid_ref[:, i * cut : (i + 1) * cut].astype(jnp.float32) + mixed
            after[:, i * cut : (i + 1) * cut] = piece.astype(jnp.bfloat16)
        xg[z, c, x] = rms_scale(after[...], gain_ref[...]).astype(jnp.bfloat16)

    piece_rows = rows // HALVES

    def xi(i):
        return (x - i + nx) % nx

    def piece(a, cc, xx, h):
        return xg.at[a, cc, xx, pl.ds(h * piece_rows, piece_rows)]

    def hop(a, h, send_sem, to):
        return lambda: (
            piece(a, c, x, h), piece(a, c, x, h), send_sem(), bz_r.at[a, h], at(to(), y, x, c)
        )

    def bx(a, i, h, xx):
        return lambda: (
            piece(a, c, xx(i), h), piece(a, c, xx(i), h), bx_s.at[a, i, h], bx_r.at[a, i, h], xdev[i]
        )

    def bc(a, i, h, cc):
        return lambda: (
            piece(a, cc, xi(i), h), piece(a, cc, xi(i), h),
            bc_s.at[a, i, h], bc_r.at[a, i, h], partner,
        )

    def own_x(i):
        return x

    def spread(a, h):
        for i in range(1, nx):
            start(bx(a, i, h, own_x))
        start(bc(a, 0, h, c))

    for h in range(HALVES):
        under(z + 1 < nz, lambda h=h: start(hop(z, h, lambda: bz_s.at[z, h], lambda: z + 1)))
        under(z > 0, lambda h=h: start(hop(z, h, lambda: bo_s.at[h], lambda: z - 1)))
        spread(z, h)

    def from_z(i):
        a = turns[i]
        after_me = z + 2 * jnp.minimum(jnp.maximum(z - a, 0), 1) - 1
        onward = (after_me >= 0) & (after_me < nz)
        for h in range(HALVES):
            arrive(hop(a, h, lambda: bz_s.at[a, h], lambda: z))
            under(
                onward, lambda h=h: start(hop(a, h, lambda: bz_s.at[a, h], lambda: after_me))
            )
            spread(a, h)

    def from_x(i):
        a = turns[i]
        for h in range(HALVES):
            for j in range(1, nx):
                arrive(bx(a, j, h, xi))
                start(bc(a, j, h, c))

    def rows_here(a):
        for h in range(HALVES):
            for j in range(nx):
                arrive(bc(a, j, h, 1 - c))

    def weights_here(out, sy, ry):
        for a in range(nz):
            for j in range(1, ny):
                slot = lambda: out.at[a * ny + (y - j + ny) % ny]
                arrive(lambda: (slot(), slot(), sy.at[a, j], ry.at[a, j], ydev[j]))

    def up_step(i):
        a = turns[i]
        rows_here(a)
        tokens = xg[a].reshape(tp * rows, width)
        projected = jnp.dot(
            tokens, up_out[...].reshape(width, units), preferred_element_type=jnp.float32
        )
        hid[a] = jnp.square(jnp.maximum(projected, 0.0)).astype(jnp.bfloat16)

    def down_step(k):
        hidden = hid[turns[k]]
        cols = dn_out.shape[2]
        for b in range(dn_out.shape[0]):
            out = jnp.dot(hidden, dn_out[b], preferred_element_type=jnp.float32)
            pbuf[k, :, :, :, b * cols : (b + 1) * cols] = out.astype(jnp.bfloat16).reshape(
                CORES, nx, rows, cols
            )
        start(lambda: (pbuf.at[k, 1 - c], cbuf.at[k], cc_s.at[k], cc_r.at[k], partner))

    def core_sum(k):
        arrive(lambda: (cbuf.at[k], cbuf.at[k], cc_s.at[k], cc_r.at[k], partner))
        pbuf[k, c] = (
            pbuf[k, c].astype(jnp.float32) + cbuf[k].astype(jnp.float32)
        ).astype(jnp.bfloat16)
        for j in range(1, nx):
            start(
                lambda j=j: (
                    pbuf.at[k, c, (x + j) % nx], xbuf.at[k, j], cx_s.at[k, j], cx_r.at[k, j], xdev[j]
                )
            )

    def cross_sum(k):
        summed = pbuf[k, c, x].astype(jnp.float32)
        for j in range(1, nx):
            arrive(lambda: (xbuf.at[k, j], xbuf.at[k, j], cx_s.at[k, j], cx_r.at[k, j], xdev[j]))
            summed = summed + xbuf[k, j].astype(jnp.float32)
        zsend[k] = summed.astype(jnp.bfloat16)
        if k:
            start(lambda: (zsend.at[k], zbuf.at[z], cz_s.at[k], cz_r.at[z], zabs[k]))

    with jax.named_scope("fwd3"):
        dn_forward(nz - 1)
    with jax.named_scope("g_x"):
        from_x(0)
    if nz > 2:
        with jax.named_scope("g_z"):
            from_z(1)
    with jax.named_scope("fwd4"):
        for i in far_first[1:]:
            dn_forward(i)
    local[6].wait()
    local[7].wait()
    with jax.named_scope("w_up"):
        weights_here(up_out, uy_s, uy_r)
    with jax.named_scope("up"):
        up_step(0)
    for i in range(1, nz - 1):
        with jax.named_scope("g_x"):
            from_x(i)
        if i + 1 < nz - 1:
            with jax.named_scope("g_z"):
                from_z(i + 1)
        with jax.named_scope("up"):
            up_step(i)
    late = [nz - 1] if nz > 1 else []
    for i in late:
        with jax.named_scope("g_z"):
            from_z(i)
    with jax.named_scope("w_dn"):
        weights_here(dn_out, dy_s, dy_r)
    order = list(range(nz - 2, 0, -1)) + late + [0]
    for i in order[:-2]:
        with jax.named_scope("down"):
            down_step(i)
    with jax.named_scope("core"):
        for i in order[:-2]:
            core_sum(i)
    for i in late:
        with jax.named_scope("g_x"):
            from_x(i)
        with jax.named_scope("up"):
            up_step(i)
        with jax.named_scope("down"):
            down_step(i)
    with jax.named_scope("down"):
        down_step(0)
    with jax.named_scope("core"):
        for i in late + [0]:
            core_sum(i)
    for i in order:
        with jax.named_scope("cross"):
            cross_sum(i)
    with jax.named_scope("final"):
        final = after[...].astype(jnp.float32)
        ffn = zsend[0].astype(jnp.float32)
        for k in range(1, nz):
            a = turns[k]
            arrive(lambda: (zbuf.at[a], zbuf.at[a], cz_s.at[k], cz_r.at[a], zabs[k]))
            ffn = ffn + zbuf[a].astype(jnp.float32)
        out_ref[...] = (final + ffn).astype(jnp.bfloat16)

    with jax.named_scope("wait_send"):
        drain()


def layer(
    ny, nz, nx, q_lat, kv_lat, rope_key, cos, sin, q_gain, kv_gain, gain, resid,
    wqs, wql, wks, wkl, wos, wol, w_up, w_down,
):
    tp, sp = nx * CORES, ny * nz
    rows, width = resid.shape
    tok_rows, rank = kv_lat.shape
    small = wks.shape[1] // (2 * SMALL_DIM)
    large = wkl.shape[1] // (2 * LARGE_DIM)
    heads = small + large
    units = w_up.shape[1] // nz
    query_cols = -(-max(wqs.shape[0], wql.shape[0]) // LANES) * LANES
    dma = pltpu.SemaphoreType.DMA
    vmem = pl.BlockSpec(memory_space=pltpu.VMEM)
    anywhere = pl.BlockSpec(memory_space=pl.ANY)
    b16, f32 = jnp.bfloat16, jnp.float32

    def pair(*shape):
        return [dma(shape), dma(shape)]

    def like(array):
        return pltpu.VMEM(array.shape, array.dtype)

    return pl.pallas_call(
        functools.partial(layer_kernel, ny, nz, nx),
        out_shape=jax.ShapeDtypeStruct((rows, width), b16),
        in_specs=[vmem] * 9 + [anywhere] * 8,
        out_specs=vmem,
        scratch_shapes=[
            pltpu.VMEM((sp, tok_rows, rank + LANES), b16),
            pltpu.VMEM((sp, w_up.shape[0], units), b16),
            pltpu.VMEM((sp, units, w_down.shape[1]), b16),
            like(wqs),
            like(wql),
            like(wks),
            like(wkl),
            like(wos),
            like(wol),
            pltpu.VMEM((LANES, tok_rows), f32),
            pltpu.VMEM((tok_rows, query_cols), f32),
            pltpu.VMEM((heads, tok_rows, 2 * LANES), b16),
            pltpu.VMEM((heads, tok_rows, 1), f32),
            pltpu.VMEM((heads, tok_rows, 1), f32),
            pltpu.VMEM((heads, tok_rows, LARGE_DIM), f32),
            pltpu.VMEM((HALVES, CORES, nx, rows, width // HALVES), b16),
            pltpu.VMEM((HALVES, nx, rows, width // HALVES), b16),
            pltpu.VMEM((HALVES, nx, rows, width // HALVES), b16),
            pltpu.VMEM((rows, width), b16),
            pltpu.VMEM((nz, CORES, nx, rows, width), b16),
            pltpu.VMEM((nz, tp * rows, units), b16),
            pltpu.VMEM((nz, CORES, nx, rows, width), b16),
            pltpu.VMEM((nz, nx, rows, width), b16),
            pltpu.VMEM((nz, nx, rows, width), b16),
            pltpu.VMEM((nz, rows, width), b16),
            pltpu.VMEM((nz, rows, width), b16),
            dma((8,)),
            pltpu.SemaphoreType.REGULAR,
        ]
        + pair(nz)
        + pair(nz, ny)
        + pair(nz, ny, nx) * 2
        + (pair(nz) + pair(nz, ny)) * 2
        + pair(HALVES)
        + pair(HALVES, nx)
        + pair(nz, HALVES)
        + [dma((HALVES,))]
        + pair(nz, nx, HALVES) * 2
        + pair(nz)
        + pair(nz, nx)
        + pair(nz),
        compiler_params=pltpu.CompilerParams(
            collective_id=1, has_side_effects=True, vmem_limit_bytes=63 * 2**20
        ),
        name="layer",
    )(
        q_lat, kv_lat, rope_key, cos, sin, q_gain, kv_gain, gain, resid,
        wqs, wql, wks, wkl, wos, wol, w_up, w_down,
    )


def on_device(
    ny,
    nz,
    nx,
    resid,
    q_latent,
    kv_latent,
    rope_key,
    q_gain,
    kv_gain,
    w_q_small,
    w_q_large,
    w_kv_small,
    w_kv_large,
    w_out_small,
    w_out_large,
    ffn_gain,
    w_up,
    w_down,
):
    tok_rows = q_latent.shape[0]
    offset = lax.axis_index("sp") * tok_rows
    cos, sin = rotary_tables(offset + jnp.arange(tok_rows, dtype=jnp.int32))
    return layer(
        ny,
        nz,
        nx,
        q_latent,
        kv_latent,
        rope_key.T,
        cos,
        sin,
        q_gain.reshape(-1, LANES),
        kv_gain.reshape(1, -1),
        ffn_gain.reshape(1, -1),
        resid,
        w_q_small.T,
        w_q_large.T,
        w_kv_small,
        w_kv_large,
        w_out_small,
        w_out_large,
        w_up,
        w_down,
    )


def solution(mesh):
    ny = inner_split(mesh.shape["sp"])
    nz = mesh.shape["sp"] // ny
    nx = mesh.shape["tp"] // CORES
    return jax.shard_map(
        functools.partial(on_device, ny, nz, nx),
        mesh=mesh,
        in_specs=(
            P(("sp", "tp"), None),
            P("sp", None),
            P("sp", None),
            P("sp", None),
            P(),
            P(),
            P(None, "tp"),
            P(None, "tp"),
            P(None, "tp"),
            P(None, "tp"),
            P("tp", None),
            P("tp", None),
            P(),
            P("sp", "tp"),
            P("tp", "sp"),
        ),
        out_specs=P(("sp", "tp"), None),
        check_vma=False,
    )
```

```python
import functools

import jax
import jax.numpy as jnp
from jax import lax
from jax.experimental import pallas as pl
from jax.experimental.pallas import tpu as pltpu
from jax.sharding import PartitionSpec as P

SMALL_DIM = 64
LARGE_DIM = 128
ROPE_DIM = 32
HALF_ROPE = ROPE_DIM // 2

epsilon = 1e-06
theta_base = 10000.0
LOG2E = 1.4426950408889634

MESH = pl.DeviceIdType.MESH
CORES = 2
LANES = 128
HALVES = 2


def rms_scale(inputs, gain_vec):
    values = inputs.astype(jnp.float32)
    return (
        values * lax.rsqrt(jnp.mean(values * values, axis=-1, keepdims=True) + epsilon) * gain_vec
    )


def rotary_tables(positions):
    exponent = jnp.arange(0, ROPE_DIM, 2, dtype=jnp.float32) / ROPE_DIM
    angles = (theta_base ** (-exponent))[:, None] * positions.astype(jnp.float32)[None, :]
    return jnp.cos(angles), jnp.sin(angles)


def inner_split(count):
    best = 1
    for size in range(1, count + 1):
        if size * size <= count and count % size == 0:
            best = size
    return best


def outward(count, z, i):
    orders = [
        sorted(range(count), key=lambda a: (abs(a - zz), a if 2 * zz < count else -a))
        for zz in range(count)
    ]
    got = orders[0][i]
    for zz in range(1, count):
        got = got + jnp.minimum(jnp.maximum(z - (zz - 1), 0), 1) * (orders[zz][i] - orders[zz - 1][i])
    return got


def remote(src, dst, send_sem, recv_sem, device):
    return pltpu.make_async_remote_copy(
        src_ref=src,
        dst_ref=dst,
        send_sem=send_sem,
        recv_sem=recv_sem,
        device_id=device,
        device_id_type=MESH,
    )


def place(ny, nz, nx):
    s, t = lax.axis_index("sp"), lax.axis_index("tp")
    z, y = s // ny, s % ny
    x, c = t // CORES, t % CORES

    def at(zz, yy, xx, cc):
        return (zz * ny + yy, xx * CORES + cc)

    return z, y, x, c, at


def layer_kernel(
    ny, nz, nx,
    q_lat, kv_lat, rope_t, cos_t, sin_t, q_gain, kv_gain, gain_ref, resid_ref,
    wqs_hbm, wql_hbm, wks_hbm, wkl_hbm, wos_hbm, wol_hbm, up_ref, dn_ref, out_ref,
    lat_out, up_out, dn_out, wqs, wql, wks, wkl, wos, wol, stood, spread_ref, q_all,
    row_max, row_sum, weighted, part_ref, rs_c, rs_x, after, xg, hid,
    pbuf, cbuf, xbuf, zsend, zbuf, ebuf, own_sem, go_sem,
    lz_s, lz_r, ly_s, ly_r, lx_s, lx_r, lc_s, lc_r,
    uz_s, uz_r, uy_s, uy_r, dz_s, dz_r, dy_s, dy_r,
    ac_s, ac_r, ax_s, ax_r, bz_s, bz_r, bo_s, bx_s, bx_r, bc_s, bc_r,
    cc_s, cc_r, cx_s, cx_r, cz_s, cz_r, ez_r,
):
    z, y, x, c, at = place(ny, nz, nx)
    s = z * ny + y
    tp = nx * CORES
    t = x * CORES + c
    tok_rows = lat_out.shape[1]
    part = tok_rows // tp
    rank = kv_lat.shape[1]
    units = up_out.shape[2]
    rows, width = resid_ref.shape
    heads = q_all.shape[0]
    small = wks.shape[1] // (2 * SMALL_DIM)
    partner = at(z, y, x, 1 - c)
    zdev = [at((z + k) % nz, y, x, c) for k in range(nz)]
    ydev = [at(z, (y + j) % ny, x, c) for j in range(ny)]
    xdev = [at(z, y, (x + i) % nx, c) for i in range(nx)]
    turns = [outward(nz, z, i) for i in range(nz)]
    zabs = [at(a, y, x, c) for a in turns]
    far_first = list(range(nz - 1, 0, -1))

    barrier = pltpu.get_barrier_semaphore()
    friends = zdev[1:] + ydev[1:] + xdev[1:] + [partner]
    for device in friends:
        pl.semaphore_signal(barrier, inc=1, device_id=device, device_id_type=MESH)

    def up_part(to):
        return up_ref.at[:, pl.ds(pl.multiple_of(to * units, LANES), units)]

    def dn_part(to):
        first = to * units
        if not isinstance(first, int):
            first = pl.multiple_of(first, LANES)
        return dn_ref.at[pl.ds(first, units), :]

    local = [
        pltpu.make_async_copy(src, dst, own_sem.at[i])
        for i, (src, dst) in enumerate(
            (
                (wqs_hbm, wqs),
                (wql_hbm, wql),
                (wks_hbm, wks),
                (wkl_hbm, wkl),
                (wos_hbm, wos),
                (wol_hbm, wol),
                (up_part(z), up_out.at[s]),
                (dn_part(z), dn_out.at[s]),
            )
        )
    ]
    for copy in local:
        copy.start()

    sent = []
    guard = [None]

    def finish(make):
        remote(*make()).wait_send()

    def drain():
        for condition, make in sent:
            if condition is None:
                finish(make)
            else:
                pl.when(condition)(functools.partial(finish, make))
        sent.clear()

    def start(make):
        sent.append((guard[-1], make))
        remote(*make()).start()

    def under(condition, body):
        guard.append(condition)
        pl.when(condition)(body)
        guard.pop()

    def arrive(make):
        remote(*make()).wait_recv()

    def zi(k):
        return (z - k + nz) % nz

    def block(k, j):
        return zi(k) * ny + (y - j + ny) % ny

    lane = lax.broadcasted_iota(jnp.int32, (tok_rows, LANES), 1)

    low = rope_t[:HALF_ROPE].astype(jnp.float32)
    high = rope_t[HALF_ROPE:].astype(jnp.float32)
    cos, sin = cos_t[...], sin_t[...]
    stood[...] = jnp.zeros_like(stood)
    stood[:HALF_ROPE] = low * cos - high * sin
    stood[HALF_ROPE:ROPE_DIM] = high * cos + low * sin
    lat_out[s, :, rank:] = stood[...].T.astype(jnp.bfloat16)
    lat_out[s, :, :rank] = rms_scale(kv_lat[...], kv_gain[...]).astype(jnp.bfloat16)

    with jax.named_scope("greet"):
        pl.semaphore_wait(barrier, len(friends))

    def share(b, p):
        return lat_out.at[b, pl.ds(pl.multiple_of(p * part, part), part)]

    def at_part(i, cc):
        return ((x - i + nx) % nx) * CORES + cc

    def lz(k, b):
        return lambda: (share(b(), t), share(b(), t), lz_s.at[k], lz_r.at[k], zdev[k])

    def ly(k, j, b):
        return lambda: (share(b(), t), share(b(), t), ly_s.at[k, j], ly_r.at[k, j], ydev[j])

    def lx(k, j, i, p):
        return lambda: (
            share(block(k, j), p()), share(block(k, j), p()),
            lx_s.at[k, j, i], lx_r.at[k, j, i], xdev[i],
        )

    def lc(k, j, i, cc):
        return lambda: (
            share(block(k, j), at_part(i, cc)), share(block(k, j), at_part(i, cc)),
            lc_s.at[k, j, i], lc_r.at[k, j, i], partner,
        )

    def lat_spread(k, j):
        for i in range(1, nx):
            start(lx(k, j, i, lambda: t))
        start(lc(k, j, 0, c))

    for k in range(1, nz):
        under(z + k < nz, lambda k=k: start(lz(k, lambda: s)))
    for j in range(1, ny):
        under(y + j < ny, lambda j=j: start(ly(0, j, lambda: s)))

    def z_up(i):
        a = turns[i]
        return lambda: (up_part(a), up_out.at[s], uz_s.at[i], uz_r.at[z], zabs[i])

    def z_dn(i):
        a = turns[i]
        return lambda: (dn_part(a), dn_out.at[s], dz_s.at[i], dz_r.at[z], zabs[i])

    def forward(i, out, zs, zr, ys, yr):
        a = turns[i]
        slot = lambda: out.at[a * ny + y]
        arrive(lambda: (slot(), slot(), zs.at[i], zr.at[a], zabs[i]))
        for j in range(1, ny):
            start(lambda j=j: (slot(), slot(), ys.at[a, j], yr.at[a, j], ydev[j]))

    def up_forward(i):
        forward(i, up_out, uz_s, uz_r, uy_s, uy_r)

    def dn_forward(i):
        forward(i, dn_out, dz_s, dz_r, dy_s, dy_r)

    with jax.named_scope("queries"):
        stood[:HALF_ROPE] = cos
        stood[HALF_ROPE:ROPE_DIM] = cos
        cos_ref = stood[...].T
        stood[:HALF_ROPE] = -sin
        stood[HALF_ROPE:ROPE_DIM] = sin
        sin_ref = stood[...].T

        def turn(values):
            swapped = jnp.where(
                lane < HALF_ROPE,
                pltpu.roll(values, LANES - HALF_ROPE, 1),
                pltpu.roll(values, HALF_ROPE, 1),
            )
            turned = values * cos_ref + swapped * sin_ref
            return jnp.where(lane < ROPE_DIM, turned, 0.0)

        spread_ref[...] = jnp.zeros_like(spread_ref)
        values = q_lat[...].astype(jnp.float32)
        values = values * lax.rsqrt(jnp.mean(values * values, axis=-1, keepdims=True) + epsilon)
        query_normed = jnp.concatenate(
            [
                values[:, b * LANES : (b + 1) * LANES] * q_gain[b : b + 1]
                for b in range(values.shape[1] // LANES)
            ],
            axis=1,
        ).astype(jnp.bfloat16)
        head = 0
        for w_ref, copies, nope in ((wqs, local[0], SMALL_DIM), (wql, local[1], LARGE_DIM)):
            copies.wait()
            cols = w_ref.shape[0]
            spread_ref[:, :cols] = lax.dot_general(
                query_normed,
                w_ref[...],
                (((1,), (1,)), ((), ())),
                preferred_element_type=jnp.float32,
            )

            def take(first, size):
                b, off = first // LANES, first % LANES
                got = spread_ref[:, b * LANES : (b + 1) * LANES]
                if off:
                    got = pltpu.roll(got, LANES - off, 1)
                if off + size > LANES:
                    more = spread_ref[:, (b + 1) * LANES : (b + 2) * LANES]
                    got = jnp.where(lane < LANES - off, got, pltpu.roll(more, LANES - off, 1))
                return got

            for h in range(cols // (nope + ROPE_DIM)):
                first = h * (nope + ROPE_DIM)
                content = take(first, nope)
                if nope < LANES:
                    content = jnp.where(lane < nope, content, 0.0)
                q_all[head, :, :LANES] = content.astype(jnp.bfloat16)
                q_all[head, :, LANES:] = turn(take(first + nope, ROPE_DIM)).astype(jnp.bfloat16)
                head += 1
    local[2].wait()
    local[3].wait()

    def attend(latents, causal, first):
        latent = latents[:, :rank]
        turned = latents[:, rank:]
        kv_small = jnp.dot(latent, wks[...], preferred_element_type=jnp.float32)
        kv_small = kv_small.astype(jnp.bfloat16)
        kv_large = jnp.dot(latent, wkl[...], preferred_element_type=jnp.float32)
        kv_large = kv_large.astype(jnp.bfloat16)
        for h in range(heads):
            if h < small:
                key = kv_small[:, 2 * SMALL_DIM * h : 2 * SMALL_DIM * (h + 1)]
                value = key
                scale = (SMALL_DIM + ROPE_DIM) ** (-0.5)
            else:
                begin = 2 * LARGE_DIM * (h - small)
                key = kv_large[:, begin : begin + LARGE_DIM]
                value = kv_large[:, begin + LARGE_DIM : begin + 2 * LARGE_DIM]
                scale = (LARGE_DIM + ROPE_DIM) ** (-0.5)
            scores = lax.dot_general(
                q_all[h],
                jnp.concatenate([key, turned], axis=1),
                (((1,), (1,)), ((), ())),
                preferred_element_type=jnp.float32,
            )
            scores = scores * (scale * LOG2E)
            if causal is not None:
                scores = jnp.where(causal, scores, -1e30)
            top = jnp.max(scores, axis=-1, keepdims=True)
            if first:
                weights = jnp.exp2(scores - top)
                row_max[h] = top
                row_sum[h] = jnp.sum(weights, axis=-1, keepdims=True)
                weighted[h] = jnp.dot(
                    weights.astype(jnp.bfloat16), value, preferred_element_type=jnp.float32
                )
                continue
            old_max = row_max[h]
            new_max = jnp.maximum(old_max, top)
            shrink = jnp.exp2(old_max - new_max)
            weights = jnp.exp2(scores - new_max)
            row_max[h] = new_max
            row_sum[h] = row_sum[h] * shrink + jnp.sum(weights, axis=-1, keepdims=True)
            weighted[h] = weighted[h] * shrink + jnp.dot(
                weights.astype(jnp.bfloat16), value, preferred_element_type=jnp.float32
            )

    def lat_from_z(k):
        slot = lambda: block(k, 0)
        arrive(lz(k, slot))
        for j in range(1, ny):
            start(ly(k, j, slot))
        lat_spread(k, 0)

    def lat_from_y(k, j):
        arrive(ly(k, j, lambda: block(k, j)))
        lat_spread(k, j)

    def lat_from_x(k, j):
        for i in range(1, nx):
            arrive(lx(k, j, i, lambda i=i: at_part(i, c)))
            start(lc(k, j, i, c))

    def lat_here(k, j):
        for i in range(nx):
            arrive(lc(k, j, i, 1 - c))

    with jax.named_scope("own"):
        ahead = lax.broadcasted_iota(jnp.int32, (tok_rows, tok_rows), 1) <= (
            lax.broadcasted_iota(jnp.int32, (tok_rows, tok_rows), 0)
        )
        attend(lat_out[s], ahead, True)
    with jax.named_scope("drain"):
        drain()
        pl.semaphore_signal(go_sem, inc=1, device_id=partner, device_id_type=MESH)
        pl.semaphore_wait(go_sem, 1)
    for i in far_first:
        start(z_up(i))
    for i in far_first:
        start(z_dn(i))
    for j in range(1, ny):
        start(lambda j=j: (up_part(z), up_out.at[s], uy_s.at[z, j], uy_r.at[z, j], ydev[j]))
    with jax.named_scope("lat_z"):
        for k in range(1, nz):
            under(z >= k, lambda k=k: lat_from_z(k))
        for j in range(1, ny):
            under(y >= j, lambda j=j: lat_from_y(0, j))
    with jax.named_scope("lat_x0"):
        for j in range(1, ny):
            under(y >= j, lambda j=j: lat_from_x(0, j))
        for k in range(1, nz):
            under(z >= k, lambda k=k: lat_from_x(k, 0))
    with jax.named_scope("lat_c0"):
        for j in range(1, ny):
            under(y >= j, lambda j=j: lat_here(0, j))
    with jax.named_scope("near"):
        def near(j, carry):
            attend(lat_out[z * ny + j], None, False)
            return carry

        lax.fori_loop(0, y, near, 0)
    with jax.named_scope("lat_y"):
        for k in range(1, nz):
            for j in range(1, ny):
                under(z >= k, lambda k=k, j=j: lat_from_y(k, j))
        for k in range(1, nz):
            for j in range(1, ny):
                under(z >= k, lambda k=k, j=j: lat_from_x(k, j))
    for j in range(1, ny):
        start(lambda j=j: (dn_part(z), dn_out.at[s], dy_s.at[z, j], dy_r.at[z, j], ydev[j]))
    with jax.named_scope("up_fwd"):
        for i in far_first[:1]:
            up_forward(i)
    with jax.named_scope("lat_all"):
        for k in range(1, nz):
            for j in range(ny):
                under(z >= k, lambda k=k, j=j: lat_here(k, j))
    with jax.named_scope("far"):
        def far(zz, carry):
            latents = lat_out[pl.ds(zz * ny, ny)].reshape(ny * tok_rows, lat_out.shape[2])
            attend(latents, None, False)
            return carry

        lax.fori_loop(0, z, far, 0)
    local[4].wait()
    local[5].wait()
    with jax.named_scope("outproj"):
        parts = []
        for h in range(heads):
            head_out = (weighted[h] / row_sum[h]).astype(jnp.bfloat16)
            parts.append(head_out[:, SMALL_DIM:] if h < small else head_out)
        from_small = jnp.concatenate(parts[:small], axis=1)
        from_large = jnp.concatenate(parts[small:], axis=1)
        cut = width // HALVES

        def ac(i):
            return lambda: (part_ref.at[i, 1 - c], rs_c.at[i], ac_s.at[i], ac_r.at[i], partner)

        def ax(i, j):
            return lambda: (
                part_ref.at[i, c, (x + j) % nx], rs_x.at[i, j], ax_s.at[i, j], ax_r.at[i, j], xdev[j]
            )

        for i in range(HALVES):
            mixed = jnp.dot(
                from_small, wos[:, i * cut : (i + 1) * cut], preferred_element_type=jnp.float32
            ) + jnp.dot(
                from_large, wol[:, i * cut : (i + 1) * cut], preferred_element_type=jnp.float32
            )
            mixed = mixed.astype(jnp.bfloat16)
            for xx in range(nx):
                for cc in range(CORES):
                    first = (xx * CORES + cc) * rows
                    part_ref[i, cc, xx] = mixed[first : first + rows]
            start(ac(i))
    with jax.named_scope("rs_core"):
        for i in range(HALVES):
            arrive(ac(i))
            part_ref[i, c] = (
                part_ref[i, c].astype(jnp.float32) + rs_c[i].astype(jnp.float32)
            ).astype(jnp.bfloat16)
            for j in range(1, nx):
                start(ax(i, j))
    with jax.named_scope("fwd2"):
        for i in far_first[1:]:
            up_forward(i)
    with jax.named_scope("rs_x"):
        for i in range(HALVES):
            mixed = part_ref[i, c, x].astype(jnp.float32)
            for j in range(1, nx):
                arrive(ax(i, j))
                mixed = mixed + rs_x[i, j].astype(jnp.float32)
            piece = resid_ref[:, i * cut : (i + 1) * cut].astype(jnp.float32) + mixed
            after[:, i * cut : (i + 1) * cut] = piece.astype(jnp.bfloat16)
        xg[z, c, x] = rms_scale(after[...], gain_ref[...]).astype(jnp.bfloat16)

    piece_rows = rows // HALVES

    def xi(i):
        return (x - i + nx) % nx

    def piece(a, cc, xx, h):
        return xg.at[a, cc, xx, pl.ds(h * piece_rows, piece_rows)]

    def hop(a, h, send_sem, to):
        return lambda: (
            piece(a, c, x, h), piece(a, c, x, h), send_sem(), bz_r.at[a, h], at(to(), y, x, c)
        )

    def bx(a, i, h, xx):
        return lambda: (
            piece(a, c, xx(i), h), piece(a, c, xx(i), h), bx_s.at[a, i, h], bx_r.at[a, i, h], xdev[i]
        )

    def bc(a, i, h, cc):
        return lambda: (
            piece(a, cc, xi(i), h), piece(a, cc, xi(i), h),
            bc_s.at[a, i, h], bc_r.at[a, i, h], partner,
        )

    def own_x(i):
        return x

    def spread(a, h):
        for i in range(1, nx):
            start(bx(a, i, h, own_x))
        start(bc(a, 0, h, c))

    for h in range(HALVES):
        under(z + 1 < nz, lambda h=h: start(hop(z, h, lambda: bz_s.at[z, h], lambda: z + 1)))
        under(z > 0, lambda h=h: start(hop(z, h, lambda: bo_s.at[h], lambda: z - 1)))
        spread(z, h)

    after_me = [z + 2 * jnp.minimum(jnp.maximum(z - a, 0), 1) - 1 for a in turns]
    onward = [(a >= 0) & (a < nz) for a in after_me]

    def from_z(i, relay=True):
        a = turns[i]
        for h in range(HALVES):
            arrive(hop(a, h, lambda: bz_s.at[a, h], lambda: z))
            if relay:
                under(
                    onward[i],
                    lambda h=h: start(hop(a, h, lambda: bz_s.at[a, h], lambda: after_me[i])),
                )
            spread(a, h)

    def from_x(i):
        a = turns[i]
        for h in range(HALVES):
            for j in range(1, nx):
                arrive(bx(a, j, h, xi))
                start(bc(a, j, h, c))

    def rows_here(a):
        for h in range(HALVES):
            for j in range(nx):
                arrive(bc(a, j, h, 1 - c))

    def from_y(p, out, sy, ry):
        a = turns[p]
        for j in range(1, ny):
            slot = lambda: out.at[a * ny + (y - j + ny) % ny]
            arrive(lambda: (slot(), slot(), sy.at[a, j], ry.at[a, j], ydev[j]))

    def up_step(i):
        a = turns[i]
        rows_here(a)
        tokens = xg[a].reshape(tp * rows, width)
        projected = jnp.dot(
            tokens, up_out[...].reshape(width, units), preferred_element_type=jnp.float32
        )
        hid[a] = jnp.square(jnp.maximum(projected, 0.0)).astype(jnp.bfloat16)

    to_core, to_cross = [], []
    at_end = (z == 0) | (z == nz - 1)
    inside = jnp.logical_not(at_end)
    takes = [((z == 1) & (a > z)) | ((z == nz - 2) & (a < z)) for a in turns]
    takes = [inside & yes for yes in takes]
    alone = [inside & jnp.logical_not(yes) for yes in takes]
    apart = [
        ((a == 0) | (a == nz - 1)) & ((a - z > 1) | (z - a > 1)) for a in turns
    ]

    def inward(i, p):
        return lambda: (
            zsend.at[i, p], ebuf.at[turns[i], turns[p]],
            cz_s.at[i, p], ez_r.at[turns[i], turns[p]], zabs[1],
        )

    def outward_sum(i, p):
        return lambda: (
            zsend.at[i, p], zbuf.at[z, turns[p]],
            cz_s.at[i, p], cz_r.at[z, turns[p]], zabs[i],
        )

    def core_send(i, p):
        return lambda: (
            pbuf.at[i, p, 1 - c], cbuf.at[i, p], cc_s.at[i, p], cc_r.at[i, p], partner
        )

    def cross_send(i, p, j):
        return lambda: (
            pbuf.at[i, p, c, (x + j) % nx], xbuf.at[i, p, j],
            cx_s.at[i, p, j], cx_r.at[i, p, j], xdev[j],
        )

    def down_step(i, p):
        hidden = hid[turns[i]]
        cols = dn_out.shape[2]
        for j in range(ny):
            out = jnp.dot(hidden, dn_out[turns[p] * ny + j], preferred_element_type=jnp.float32)
            pbuf[i, p, :, :, :, j * cols : (j + 1) * cols] = out.astype(jnp.bfloat16).reshape(
                CORES, nx, rows, cols
            )
        start(core_send(i, p))

    def core_sum(i, p):
        arrive(core_send(i, p))
        pbuf[i, p, c] = (
            pbuf[i, p, c].astype(jnp.float32) + cbuf[i, p].astype(jnp.float32)
        ).astype(jnp.bfloat16)
        for j in range(1, nx):
            start(cross_send(i, p, j))

    def cross_sum(i, p):
        summed = pbuf[i, p, c, x].astype(jnp.float32)
        for j in range(1, nx):
            arrive(cross_send(i, p, j))
            summed = summed + xbuf[i, p, j].astype(jnp.float32)
        summed = summed.astype(jnp.bfloat16)
        if i > 1:
            zsend[i, p] = summed
            under(at_end, lambda: start(inward(i, p)))
            under(alone[i], lambda: start(outward_sum(i, p)))
        elif i:
            zsend[i, p] = summed
            start(outward_sum(i, p))
        else:
            zbuf[z, turns[p]] = summed

    def combine(i, p):
        def add():
            arrive(inward(i, p))
            zsend[i, p] = (
                zsend[i, p].astype(jnp.float32)
                + ebuf[turns[i], turns[p]].astype(jnp.float32)
            ).astype(jnp.bfloat16)
            start(outward_sum(i, p))

        under(takes[i], add)

    def advance(core_lag, cross_lag):
        while len(to_core) > core_lag:
            job = to_core.pop(0)
            core_sum(*job)
            to_cross.append(job)
        while len(to_cross) > cross_lag:
            cross_sum(*to_cross.pop(0))

    def jobs(these):
        for job in these:
            down_step(*job)
            to_core.append(job)
            advance(2, 5)
        advance(0, 5)

    with jax.named_scope("fwd3"):
        dn_forward(nz - 1)
    with jax.named_scope("g_x"):
        from_x(0)
    if nz > 2:
        with jax.named_scope("g_z"):
            from_z(1)
    for i in range(2, nz - 1):
        with jax.named_scope("g_z"):
            under(inside, lambda i=i: from_z(i))
    with jax.named_scope("fwd4"):
        for i in far_first[1:]:
            dn_forward(i)
    late = [nz - 1] if nz > 1 else []
    local[6].wait()
    local[7].wait()
    with jax.named_scope("w_up"):
        for p in range(nz):
            from_y(p, up_out, uy_s, uy_r)
    with jax.named_scope("up"):
        up_step(0)
    first_in = [0] + late
    rest = list(range(nz - 2, 0, -1))
    with jax.named_scope("w_dn0"):
        for p in first_in:
            from_y(p, dn_out, dy_s, dy_r)
    with jax.named_scope("jobs"):
        jobs([(0, p) for p in first_in])
    for i in range(1, nz - 1):
        with jax.named_scope("g_x"):
            from_x(i)
        if i == nz - 2:
            with jax.named_scope("g_z"):
                under(at_end, lambda i=i: from_z(i + 1, False))
        with jax.named_scope("up"):
            up_step(i)
        with jax.named_scope("jobs"):
            jobs([(i, p) for p in first_in])
        if i < nz - 2:
            with jax.named_scope("g_z"):
                under(at_end, lambda i=i: from_z(i + 1, False))
        if i == 1:
            for n in late:
                with jax.named_scope("g_z"):
                    under(inside, lambda n=n: from_z(n))
            with jax.named_scope("w_dn"):
                for p in rest:
                    from_y(p, dn_out, dy_s, dy_r)
        with jax.named_scope("jobs"):
            jobs([(i, p) for p in rest])
    for i in late:
        with jax.named_scope("g_x"):
            from_x(i)
        with jax.named_scope("up"):
            up_step(i)
        with jax.named_scope("jobs"):
            jobs([(i, p) for p in first_in + rest])
    outer_order = [1] + list(range(nz - 1, 1, -1)) + [0]
    with jax.named_scope("jobs"):
        jobs([(0, p) for p in rest])
    waiting = [(i, p) for i in range(2, nz - 1) for p in outer_order]
    with jax.named_scope("cross"):
        while to_cross:
            advance(0, len(to_cross) - 1)
            if waiting:
                combine(*waiting.pop(0))
        for pair in waiting:
            combine(*pair)
    with jax.named_scope("comb3"):
        for i in range(max(nz - 1, 2), nz):
            for p in outer_order:
                combine(i, p)
    with jax.named_scope("final"):
        group = zbuf.shape[3]
        for p in range(nz):
            for k in range(1, nz):
                slot = lambda: zbuf.at[turns[k], p]
                make = lambda: (slot(), slot(), cz_s.at[k, p], cz_r.at[turns[k], p], zabs[k])
                if k == 1:
                    arrive(make)
                    continue

                def nothing():
                    zbuf[turns[k], p] = jnp.zeros(zbuf.shape[2:], zbuf.dtype)

                pl.when(apart[k])(nothing)
                pl.when(jnp.logical_not(apart[k]))(lambda: arrive(make))
            ffn = after[:, p * group : (p + 1) * group].astype(jnp.float32)
            for a in range(nz):
                ffn = ffn + zbuf[a, p].astype(jnp.float32)
            out_ref[:, p * group : (p + 1) * group] = ffn.astype(jnp.bfloat16)

    with jax.named_scope("wait_send"):
        drain()


def layer(
    ny, nz, nx, q_lat, kv_lat, rope_key, cos, sin, q_gain, kv_gain, gain, resid,
    wqs, wql, wks, wkl, wos, wol, w_up, w_down,
):
    tp, sp = nx * CORES, ny * nz
    rows, width = resid.shape
    tok_rows, rank = kv_lat.shape
    small = wks.shape[1] // (2 * SMALL_DIM)
    large = wkl.shape[1] // (2 * LARGE_DIM)
    heads = small + large
    units = w_up.shape[1] // nz
    query_cols = -(-max(wqs.shape[0], wql.shape[0]) // LANES) * LANES
    dma = pltpu.SemaphoreType.DMA
    vmem = pl.BlockSpec(memory_space=pltpu.VMEM)
    anywhere = pl.BlockSpec(memory_space=pl.ANY)
    b16, f32 = jnp.bfloat16, jnp.float32

    def pair(*shape):
        return [dma(shape), dma(shape)]

    def like(array):
        return pltpu.VMEM(array.shape, array.dtype)

    return pl.pallas_call(
        functools.partial(layer_kernel, ny, nz, nx),
        out_shape=jax.ShapeDtypeStruct((rows, width), b16),
        in_specs=[vmem] * 9 + [anywhere] * 8,
        out_specs=vmem,
        scratch_shapes=[
            pltpu.VMEM((sp, tok_rows, rank + LANES), b16),
            pltpu.VMEM((sp, w_up.shape[0], units), b16),
            pltpu.VMEM((sp, units, w_down.shape[1]), b16),
            like(wqs),
            like(wql),
            like(wks),
            like(wkl),
            like(wos),
            like(wol),
            pltpu.VMEM((LANES, tok_rows), f32),
            pltpu.VMEM((tok_rows, query_cols), f32),
            pltpu.VMEM((heads, tok_rows, 2 * LANES), b16),
            pltpu.VMEM((heads, tok_rows, 1), f32),
            pltpu.VMEM((heads, tok_rows, 1), f32),
            pltpu.VMEM((heads, tok_rows, LARGE_DIM), f32),
            pltpu.VMEM((HALVES, CORES, nx, rows, width // HALVES), b16),
            pltpu.VMEM((HALVES, nx, rows, width // HALVES), b16),
            pltpu.VMEM((HALVES, nx, rows, width // HALVES), b16),
            pltpu.VMEM((rows, width), b16),
            pltpu.VMEM((nz, CORES, nx, rows, width), b16),
            pltpu.VMEM((nz, tp * rows, units), b16),
            pltpu.VMEM((nz, nz, CORES, nx, rows, width // nz), b16),
            pltpu.VMEM((nz, nz, nx, rows, width // nz), b16),
            pltpu.VMEM((nz, nz, nx, rows, width // nz), b16),
            pltpu.VMEM((nz, nz, rows, width // nz), b16),
            pltpu.VMEM((nz, nz, rows, width // nz), b16),
            pltpu.VMEM((nz, nz, rows, width // nz), b16),
            dma((8,)),
            pltpu.SemaphoreType.REGULAR,
        ]
        + pair(nz)
        + pair(nz, ny)
        + pair(nz, ny, nx) * 2
        + (pair(nz) + pair(nz, ny)) * 2
        + pair(HALVES)
        + pair(HALVES, nx)
        + pair(nz, HALVES)
        + [dma((HALVES,))]
        + pair(nz, nx, HALVES) * 2
        + pair(nz, nz)
        + pair(nz, nz, nx)
        + pair(nz, nz)
        + [dma((nz, nz))],
        compiler_params=pltpu.CompilerParams(
            collective_id=1, has_side_effects=True, vmem_limit_bytes=63 * 2**20
        ),
        name="layer",
    )(
        q_lat, kv_lat, rope_key, cos, sin, q_gain, kv_gain, gain, resid,
        wqs, wql, wks, wkl, wos, wol, w_up, w_down,
    )


def on_device(
    ny,
    nz,
    nx,
    resid,
    q_latent,
    kv_latent,
    rope_key,
    q_gain,
    kv_gain,
    w_q_small,
    w_q_large,
    w_kv_small,
    w_kv_large,
    w_out_small,
    w_out_large,
    ffn_gain,
    w_up,
    w_down,
):
    tok_rows = q_latent.shape[0]
    offset = lax.axis_index("sp") * tok_rows
    cos, sin = rotary_tables(offset + jnp.arange(tok_rows, dtype=jnp.int32))
    return layer(
        ny,
        nz,
        nx,
        q_latent,
        kv_latent,
        rope_key.T,
        cos,
        sin,
        q_gain.reshape(-1, LANES),
        kv_gain.reshape(1, -1),
        ffn_gain.reshape(1, -1),
        resid,
        w_q_small.T,
        w_q_large.T,
        w_kv_small,
        w_kv_large,
        w_out_small,
        w_out_large,
        w_up,
        w_down,
    )


def solution(mesh):
    ny = inner_split(mesh.shape["sp"])
    nz = mesh.shape["sp"] // ny
    nx = mesh.shape["tp"] // CORES
    return jax.shard_map(
        functools.partial(on_device, ny, nz, nx),
        mesh=mesh,
        in_specs=(
            P(("sp", "tp"), None),
            P("sp", None),
            P("sp", None),
            P("sp", None),
            P(),
            P(),
            P(None, "tp"),
            P(None, "tp"),
            P(None, "tp"),
            P(None, "tp"),
            P("tp", None),
            P("tp", None),
            P(),
            P("sp", "tp"),
            P("tp", "sp"),
        ),
        out_specs=P(("sp", "tp"), None),
        check_vma=False,
    )
```

```python
import functools

import jax
import jax.numpy as jnp
from jax import lax
from jax.experimental import pallas as pl
from jax.experimental.pallas import tpu as pltpu
from jax.sharding import PartitionSpec as P

SMALL_DIM = 64
LARGE_DIM = 128
ROPE_DIM = 32
HALF_ROPE = ROPE_DIM // 2

epsilon = 1e-06
theta_base = 10000.0
LOG2E = 1.4426950408889634

MESH = pl.DeviceIdType.MESH
CORES = 2
LANES = 128
HALVES = 2


def rms_scale(inputs, gain_vec):
    values = inputs.astype(jnp.float32)
    return (
        values * lax.rsqrt(jnp.mean(values * values, axis=-1, keepdims=True) + epsilon) * gain_vec
    )


def rotary_tables(positions):
    exponent = jnp.arange(0, ROPE_DIM, 2, dtype=jnp.float32) / ROPE_DIM
    angles = (theta_base ** (-exponent))[:, None] * positions.astype(jnp.float32)[None, :]
    return jnp.cos(angles), jnp.sin(angles)


def inner_split(count):
    best = 1
    for size in range(1, count + 1):
        if size * size <= count and count % size == 0:
            best = size
    return best


def outward(count, z, i):
    orders = [
        sorted(range(count), key=lambda a: (abs(a - zz), a if 2 * zz < count else -a))
        for zz in range(count)
    ]
    got = orders[0][i]
    for zz in range(1, count):
        got = got + jnp.minimum(jnp.maximum(z - (zz - 1), 0), 1) * (orders[zz][i] - orders[zz - 1][i])
    return got


def remote(src, dst, send_sem, recv_sem, device):
    return pltpu.make_async_remote_copy(
        src_ref=src,
        dst_ref=dst,
        send_sem=send_sem,
        recv_sem=recv_sem,
        device_id=device,
        device_id_type=MESH,
    )


def place(ny, nz, nx):
    s, t = lax.axis_index("sp"), lax.axis_index("tp")
    z, y = s // ny, s % ny
    x, c = t // CORES, t % CORES

    def at(zz, yy, xx, cc):
        return (zz * ny + yy, xx * CORES + cc)

    return z, y, x, c, at


def layer_kernel(
    ny, nz, nx,
    q_lat, kv_lat, rope_t, cos_t, sin_t, q_gain, kv_gain, gain_ref, resid_ref,
    wqs_hbm, wql_hbm, wks_hbm, wkl_hbm, wos_hbm, wol_hbm, up_ref, dn_ref, out_ref,
    lat_out, up_out, dn_out, wqs, wql, wks, wkl, wos, wol, stood, spread_ref, q_all,
    row_max, row_sum, weighted, part_ref, rs_c, rs_x, after, xg, hid,
    pbuf, cbuf, xbuf, zsend, zbuf, ebuf, own_sem, go_sem,
    lz_s, lz_r, ly_s, ly_r, lx_s, lx_r, lc_s, lc_r,
    uz_s, uz_r, uy_s, uy_r, dz_s, dz_r, dy_s, dy_r,
    ac_s, ac_r, ax_s, ax_r, bz_s, bz_r, bo_s, bx_s, bx_r, bc_s, bc_r,
    cc_s, cc_r, cx_s, cx_r, cz_s, cz_r, ez_r,
):
    z, y, x, c, at = place(ny, nz, nx)
    s = z * ny + y
    tp = nx * CORES
    t = x * CORES + c
    tok_rows = lat_out.shape[1]
    part = tok_rows // tp
    rank = kv_lat.shape[1]
    units = up_out.shape[2]
    rows, width = resid_ref.shape
    heads = q_all.shape[0]
    small = wks.shape[1] // (2 * SMALL_DIM)
    partner = at(z, y, x, 1 - c)
    zdev = [at((z + k) % nz, y, x, c) for k in range(nz)]
    ydev = [at(z, (y + j) % ny, x, c) for j in range(ny)]
    xdev = [at(z, y, (x + i) % nx, c) for i in range(nx)]
    turns = [outward(nz, z, i) for i in range(nz)]
    zabs = [at(a, y, x, c) for a in turns]
    far_first = list(range(nz - 1, 0, -1))

    barrier = pltpu.get_barrier_semaphore()
    friends = zdev[1:] + ydev[1:] + xdev[1:] + [partner]
    for device in friends:
        pl.semaphore_signal(barrier, inc=1, device_id=device, device_id_type=MESH)

    def up_part(to):
        return up_ref.at[:, pl.ds(pl.multiple_of(to * units, LANES), units)]

    def dn_part(to):
        first = to * units
        if not isinstance(first, int):
            first = pl.multiple_of(first, LANES)
        return dn_ref.at[pl.ds(first, units), :]

    local = [
        pltpu.make_async_copy(src, dst, own_sem.at[i])
        for i, (src, dst) in enumerate(
            (
                (wqs_hbm, wqs),
                (wql_hbm, wql),
                (wks_hbm, wks),
                (wkl_hbm, wkl),
                (wos_hbm, wos),
                (wol_hbm, wol),
                (up_part(z), up_out.at[s]),
                (dn_part(z), dn_out.at[s]),
            )
        )
    ]
    for copy in local:
        copy.start()

    sent = []
    guard = [None]

    def finish(make):
        remote(*make()).wait_send()

    def drain():
        for condition, make in sent:
            if condition is None:
                finish(make)
            else:
                pl.when(condition)(functools.partial(finish, make))
        sent.clear()

    def start(make):
        sent.append((guard[-1], make))
        remote(*make()).start()

    def under(condition, body):
        guard.append(condition)
        pl.when(condition)(body)
        guard.pop()

    def arrive(make):
        remote(*make()).wait_recv()

    def zi(k):
        return (z - k + nz) % nz

    def block(k, j):
        return zi(k) * ny + (y - j + ny) % ny

    lane = lax.broadcasted_iota(jnp.int32, (tok_rows, LANES), 1)

    low = rope_t[:HALF_ROPE].astype(jnp.float32)
    high = rope_t[HALF_ROPE:].astype(jnp.float32)
    cos, sin = cos_t[...], sin_t[...]
    stood[...] = jnp.zeros_like(stood)
    stood[:HALF_ROPE] = low * cos - high * sin
    stood[HALF_ROPE:ROPE_DIM] = high * cos + low * sin
    lat_out[s, :, rank:] = stood[...].T.astype(jnp.bfloat16)
    lat_out[s, :, :rank] = rms_scale(kv_lat[...], kv_gain[...]).astype(jnp.bfloat16)

    with jax.named_scope("greet"):
        pl.semaphore_wait(barrier, len(friends))

    def share(b, p):
        return lat_out.at[b, pl.ds(pl.multiple_of(p * part, part), part)]

    def at_part(i, cc):
        return ((x - i + nx) % nx) * CORES + cc

    def lz(k, b):
        return lambda: (share(b(), t), share(b(), t), lz_s.at[k], lz_r.at[k], zdev[k])

    def ly(k, j, b):
        return lambda: (share(b(), t), share(b(), t), ly_s.at[k, j], ly_r.at[k, j], ydev[j])

    def lx(k, j, i, p):
        return lambda: (
            share(block(k, j), p()), share(block(k, j), p()),
            lx_s.at[k, j, i], lx_r.at[k, j, i], xdev[i],
        )

    def lc(k, j, i, cc):
        return lambda: (
            share(block(k, j), at_part(i, cc)), share(block(k, j), at_part(i, cc)),
            lc_s.at[k, j, i], lc_r.at[k, j, i], partner,
        )

    def lat_spread(k, j):
        for i in range(1, nx):
            start(lx(k, j, i, lambda: t))
        start(lc(k, j, 0, c))

    for k in range(1, nz):
        under(z + k < nz, lambda k=k: start(lz(k, lambda: s)))
    for j in range(1, ny):
        under(y + j < ny, lambda j=j: start(ly(0, j, lambda: s)))

    def z_up(i):
        a = turns[i]
        return lambda: (up_part(a), up_out.at[s], uz_s.at[i], uz_r.at[z], zabs[i])

    def z_dn(i):
        a = turns[i]
        return lambda: (dn_part(a), dn_out.at[s], dz_s.at[i], dz_r.at[z], zabs[i])

    def forward(i, out, zs, zr, ys, yr):
        a = turns[i]
        slot = lambda: out.at[a * ny + y]
        arrive(lambda: (slot(), slot(), zs.at[i], zr.at[a], zabs[i]))
        for j in range(1, ny):
            start(lambda j=j: (slot(), slot(), ys.at[a, j], yr.at[a, j], ydev[j]))

    def up_forward(i):
        forward(i, up_out, uz_s, uz_r, uy_s, uy_r)

    def dn_forward(i):
        forward(i, dn_out, dz_s, dz_r, dy_s, dy_r)

    with jax.named_scope("queries"):
        stood[:HALF_ROPE] = cos
        stood[HALF_ROPE:ROPE_DIM] = cos
        cos_ref = stood[...].T
        stood[:HALF_ROPE] = -sin
        stood[HALF_ROPE:ROPE_DIM] = sin
        sin_ref = stood[...].T

        def turn(values):
            swapped = jnp.where(
                lane < HALF_ROPE,
                pltpu.roll(values, LANES - HALF_ROPE, 1),
                pltpu.roll(values, HALF_ROPE, 1),
            )
            turned = values * cos_ref + swapped * sin_ref
            return jnp.where(lane < ROPE_DIM, turned, 0.0)

        spread_ref[...] = jnp.zeros_like(spread_ref)
        values = q_lat[...].astype(jnp.float32)
        values = values * lax.rsqrt(jnp.mean(values * values, axis=-1, keepdims=True) + epsilon)
        query_normed = jnp.concatenate(
            [
                values[:, b * LANES : (b + 1) * LANES] * q_gain[b : b + 1]
                for b in range(values.shape[1] // LANES)
            ],
            axis=1,
        ).astype(jnp.bfloat16)
        head = 0
        for w_ref, copies, nope in ((wqs, local[0], SMALL_DIM), (wql, local[1], LARGE_DIM)):
            copies.wait()
            cols = w_ref.shape[0]
            spread_ref[:, :cols] = lax.dot_general(
                query_normed,
                w_ref[...],
                (((1,), (1,)), ((), ())),
                preferred_element_type=jnp.float32,
            )

            def take(first, size):
                b, off = first // LANES, first % LANES
                got = spread_ref[:, b * LANES : (b + 1) * LANES]
                if off:
                    got = pltpu.roll(got, LANES - off, 1)
                if off + size > LANES:
                    more = spread_ref[:, (b + 1) * LANES : (b + 2) * LANES]
                    got = jnp.where(lane < LANES - off, got, pltpu.roll(more, LANES - off, 1))
                return got

            for h in range(cols // (nope + ROPE_DIM)):
                first = h * (nope + ROPE_DIM)
                content = take(first, nope)
                if nope < LANES:
                    content = jnp.where(lane < nope, content, 0.0)
                q_all[head, :, :LANES] = content.astype(jnp.bfloat16)
                q_all[head, :, LANES:] = turn(take(first + nope, ROPE_DIM)).astype(jnp.bfloat16)
                head += 1
    local[2].wait()
    local[3].wait()

    def attend(latents, causal, first):
        latent = latents[:, :rank]
        turned = latents[:, rank:]
        kv_small = jnp.dot(latent, wks[...], preferred_element_type=jnp.float32)
        kv_small = kv_small.astype(jnp.bfloat16)
        kv_large = jnp.dot(latent, wkl[...], preferred_element_type=jnp.float32)
        kv_large = kv_large.astype(jnp.bfloat16)
        for h in range(heads):
            if h < small:
                key = kv_small[:, 2 * SMALL_DIM * h : 2 * SMALL_DIM * (h + 1)]
                value = key
                scale = (SMALL_DIM + ROPE_DIM) ** (-0.5)
            else:
                begin = 2 * LARGE_DIM * (h - small)
                key = kv_large[:, begin : begin + LARGE_DIM]
                value = kv_large[:, begin + LARGE_DIM : begin + 2 * LARGE_DIM]
                scale = (LARGE_DIM + ROPE_DIM) ** (-0.5)
            scores = lax.dot_general(
                q_all[h],
                jnp.concatenate([key, turned], axis=1),
                (((1,), (1,)), ((), ())),
                preferred_element_type=jnp.float32,
            )
            scores = scores * (scale * LOG2E)
            if causal is not None:
                scores = jnp.where(causal, scores, -1e30)
            top = jnp.max(scores, axis=-1, keepdims=True)
            if first:
                weights = jnp.exp2(scores - top)
                row_max[h] = top
                row_sum[h] = jnp.sum(weights, axis=-1, keepdims=True)
                weighted[h] = jnp.dot(
                    weights.astype(jnp.bfloat16), value, preferred_element_type=jnp.float32
                )
                continue
            old_max = row_max[h]
            new_max = jnp.maximum(old_max, top)
            shrink = jnp.exp2(old_max - new_max)
            weights = jnp.exp2(scores - new_max)
            row_max[h] = new_max
            row_sum[h] = row_sum[h] * shrink + jnp.sum(weights, axis=-1, keepdims=True)
            weighted[h] = weighted[h] * shrink + jnp.dot(
                weights.astype(jnp.bfloat16), value, preferred_element_type=jnp.float32
            )

    def lat_from_z(k):
        slot = lambda: block(k, 0)
        arrive(lz(k, slot))
        for j in range(1, ny):
            start(ly(k, j, slot))
        lat_spread(k, 0)

    def lat_from_y(k, j):
        arrive(ly(k, j, lambda: block(k, j)))
        lat_spread(k, j)

    def lat_from_x(k, j):
        for i in range(1, nx):
            arrive(lx(k, j, i, lambda i=i: at_part(i, c)))
            start(lc(k, j, i, c))

    def lat_here(k, j):
        for i in range(nx):
            arrive(lc(k, j, i, 1 - c))

    with jax.named_scope("own"):
        ahead = lax.broadcasted_iota(jnp.int32, (tok_rows, tok_rows), 1) <= (
            lax.broadcasted_iota(jnp.int32, (tok_rows, tok_rows), 0)
        )
        attend(lat_out[s], ahead, True)
    with jax.named_scope("drain"):
        drain()
        pl.semaphore_signal(go_sem, inc=1, device_id=partner, device_id_type=MESH)
        pl.semaphore_wait(go_sem, 1)
    for i in far_first:
        start(z_up(i))
    at_end = (z == 0) | (z == nz - 1)
    inside = jnp.logical_not(at_end)
    for i in far_first:
        under(at_end, lambda i=i: start(z_dn(i)))
    for j in range(1, ny):
        start(lambda j=j: (up_part(z), up_out.at[s], uy_s.at[z, j], uy_r.at[z, j], ydev[j]))
    with jax.named_scope("lat_z"):
        for k in range(1, nz):
            under(z >= k, lambda k=k: lat_from_z(k))
        for j in range(1, ny):
            under(y >= j, lambda j=j: lat_from_y(0, j))
    with jax.named_scope("lat_x0"):
        for j in range(1, ny):
            under(y >= j, lambda j=j: lat_from_x(0, j))
        for k in range(1, nz):
            under(z >= k, lambda k=k: lat_from_x(k, 0))
    with jax.named_scope("lat_c0"):
        for j in range(1, ny):
            under(y >= j, lambda j=j: lat_here(0, j))
    with jax.named_scope("near"):
        def near(j, carry):
            attend(lat_out[z * ny + j], None, False)
            return carry

        lax.fori_loop(0, y, near, 0)
    with jax.named_scope("lat_y"):
        for k in range(1, nz):
            for j in range(1, ny):
                under(z >= k, lambda k=k, j=j: lat_from_y(k, j))
        for k in range(1, nz):
            for j in range(1, ny):
                under(z >= k, lambda k=k, j=j: lat_from_x(k, j))
    for j in range(1, ny):
        start(lambda j=j: (dn_part(z), dn_out.at[s], dy_s.at[z, j], dy_r.at[z, j], ydev[j]))
    with jax.named_scope("up_fwd"):
        for i in far_first[:1]:
            up_forward(i)
    with jax.named_scope("lat_all"):
        for k in range(1, nz):
            for j in range(ny):
                under(z >= k, lambda k=k, j=j: lat_here(k, j))
    with jax.named_scope("far"):
        def far(zz, carry):
            latents = lat_out[pl.ds(zz * ny, ny)].reshape(ny * tok_rows, lat_out.shape[2])
            attend(latents, None, False)
            return carry

        lax.fori_loop(0, z, far, 0)
    local[4].wait()
    local[5].wait()
    with jax.named_scope("outproj"):
        parts = []
        for h in range(heads):
            head_out = (weighted[h] / row_sum[h]).astype(jnp.bfloat16)
            parts.append(head_out[:, SMALL_DIM:] if h < small else head_out)
        from_small = jnp.concatenate(parts[:small], axis=1)
        from_large = jnp.concatenate(parts[small:], axis=1)
        cut = width // HALVES

        def ac(i):
            return lambda: (part_ref.at[i, 1 - c], rs_c.at[i], ac_s.at[i], ac_r.at[i], partner)

        def ax(i, j):
            return lambda: (
                part_ref.at[i, c, (x + j) % nx], rs_x.at[i, j], ax_s.at[i, j], ax_r.at[i, j], xdev[j]
            )

        for i in range(HALVES):
            mixed = jnp.dot(
                from_small, wos[:, i * cut : (i + 1) * cut], preferred_element_type=jnp.float32
            ) + jnp.dot(
                from_large, wol[:, i * cut : (i + 1) * cut], preferred_element_type=jnp.float32
            )
            mixed = mixed.astype(jnp.bfloat16)
            for xx in range(nx):
                for cc in range(CORES):
                    first = (xx * CORES + cc) * rows
                    part_ref[i, cc, xx] = mixed[first : first + rows]
            start(ac(i))
    with jax.named_scope("rs_core"):
        for i in range(HALVES):
            arrive(ac(i))
            part_ref[i, c] = (
                part_ref[i, c].astype(jnp.float32) + rs_c[i].astype(jnp.float32)
            ).astype(jnp.bfloat16)
            for j in range(1, nx):
                start(ax(i, j))
    with jax.named_scope("fwd1"):
        for i in far_first[1:][-1:]:
            up_forward(i)
    with jax.named_scope("rs_x"):
        for i in range(HALVES):
            mixed = part_ref[i, c, x].astype(jnp.float32)
            for j in range(1, nx):
                arrive(ax(i, j))
                mixed = mixed + rs_x[i, j].astype(jnp.float32)
            piece = resid_ref[:, i * cut : (i + 1) * cut].astype(jnp.float32) + mixed
            after[:, i * cut : (i + 1) * cut] = piece.astype(jnp.bfloat16)
        xg[z, c, x] = rms_scale(after[...], gain_ref[...]).astype(jnp.bfloat16)

    piece_rows = rows // HALVES

    def xi(i):
        return (x - i + nx) % nx

    def piece(a, cc, xx, h):
        return xg.at[a, cc, xx, pl.ds(h * piece_rows, piece_rows)]

    def hop(a, h, send_sem, to):
        return lambda: (
            piece(a, c, x, h), piece(a, c, x, h), send_sem(), bz_r.at[a, h], at(to(), y, x, c)
        )

    def bx(a, i, h, xx):
        return lambda: (
            piece(a, c, xx(i), h), piece(a, c, xx(i), h), bx_s.at[a, i, h], bx_r.at[a, i, h], xdev[i]
        )

    def bc(a, i, h, cc):
        return lambda: (
            piece(a, cc, xi(i), h), piece(a, cc, xi(i), h),
            bc_s.at[a, i, h], bc_r.at[a, i, h], partner,
        )

    def own_x(i):
        return x

    def spread(a, h):
        for i in range(1, nx):
            start(bx(a, i, h, own_x))
        start(bc(a, 0, h, c))

    for h in range(HALVES):
        under(z + 1 < nz, lambda h=h: start(hop(z, h, lambda: bz_s.at[z, h], lambda: z + 1)))
        under(z > 0, lambda h=h: start(hop(z, h, lambda: bo_s.at[h], lambda: z - 1)))
        spread(z, h)
    lower_inside = inside & (2 * z < nz)
    upper_inside = inside & (2 * z >= nz)
    for i in far_first:
        under(inside if i != 2 else lower_inside, lambda i=i: start(z_dn(i)))
    with jax.named_scope("fwd2"):
        for i in far_first[1:-1]:
            up_forward(i)

    after_me = [z + 2 * jnp.minimum(jnp.maximum(z - a, 0), 1) - 1 for a in turns]
    onward = [(a >= 0) & (a < nz) for a in after_me]

    def from_z(i, relay=True):
        a = turns[i]
        for h in range(HALVES):
            arrive(hop(a, h, lambda: bz_s.at[a, h], lambda: z))
            if relay:
                under(
                    onward[i],
                    lambda h=h: start(hop(a, h, lambda: bz_s.at[a, h], lambda: after_me[i])),
                )
            spread(a, h)

    def from_x(i):
        a = turns[i]
        for h in range(HALVES):
            for j in range(1, nx):
                arrive(bx(a, j, h, xi))
                start(bc(a, j, h, c))

    def rows_here(a):
        for h in range(HALVES):
            for j in range(nx):
                arrive(bc(a, j, h, 1 - c))

    def from_y(p, out, sy, ry):
        a = turns[p]
        for j in range(1, ny):
            slot = lambda: out.at[a * ny + (y - j + ny) % ny]
            arrive(lambda: (slot(), slot(), sy.at[a, j], ry.at[a, j], ydev[j]))

    def up_step(i):
        a = turns[i]
        rows_here(a)
        tokens = xg[a].reshape(tp * rows, width)
        projected = jnp.dot(
            tokens, up_out[...].reshape(width, units), preferred_element_type=jnp.float32
        )
        hid[a] = jnp.square(jnp.maximum(projected, 0.0)).astype(jnp.bfloat16)

    to_core, to_cross = [], []
    takes = [((z == 1) & (a > z)) | ((z == nz - 2) & (a < z)) for a in turns]
    takes = [inside & yes for yes in takes]
    alone = [inside & jnp.logical_not(yes) for yes in takes]
    apart = [
        ((a == 0) | (a == nz - 1)) & ((a - z > 1) | (z - a > 1)) for a in turns
    ]

    def inward(i, p):
        return lambda: (
            zsend.at[i, p], ebuf.at[turns[i], turns[p]],
            cz_s.at[i, p], ez_r.at[turns[i], turns[p]], zabs[1],
        )

    def outward_sum(i, p):
        return lambda: (
            zsend.at[i, p], zbuf.at[z, turns[p]],
            cz_s.at[i, p], cz_r.at[z, turns[p]], zabs[i],
        )

    def core_send(i, p):
        return lambda: (
            pbuf.at[i, p, 1 - c], cbuf.at[i, p], cc_s.at[i, p], cc_r.at[i, p], partner
        )

    def cross_send(i, p, j):
        return lambda: (
            pbuf.at[i, p, c, (x + j) % nx], xbuf.at[i, p, j],
            cx_s.at[i, p, j], cx_r.at[i, p, j], xdev[j],
        )

    def down_step(i, p):
        hidden = hid[turns[i]]
        cols = dn_out.shape[2]
        for j in range(ny):
            out = jnp.dot(hidden, dn_out[turns[p] * ny + j], preferred_element_type=jnp.float32)
            pbuf[i, p, :, :, :, j * cols : (j + 1) * cols] = out.astype(jnp.bfloat16).reshape(
                CORES, nx, rows, cols
            )
        start(core_send(i, p))

    def core_sum(i, p):
        arrive(core_send(i, p))
        pbuf[i, p, c] = (
            pbuf[i, p, c].astype(jnp.float32) + cbuf[i, p].astype(jnp.float32)
        ).astype(jnp.bfloat16)
        for j in range(1, nx):
            start(cross_send(i, p, j))

    def cross_sum(i, p):
        summed = pbuf[i, p, c, x].astype(jnp.float32)
        for j in range(1, nx):
            arrive(cross_send(i, p, j))
            summed = summed + xbuf[i, p, j].astype(jnp.float32)
        summed = summed.astype(jnp.bfloat16)
        if i > 1:
            zsend[i, p] = summed
            under(at_end, lambda: start(inward(i, p)))
            under(alone[i], lambda: start(outward_sum(i, p)))
        elif i:
            zsend[i, p] = summed
            start(outward_sum(i, p))
        else:
            zbuf[z, turns[p]] = summed

    def combine(i, p):
        def add():
            arrive(inward(i, p))
            zsend[i, p] = (
                zsend[i, p].astype(jnp.float32)
                + ebuf[turns[i], turns[p]].astype(jnp.float32)
            ).astype(jnp.bfloat16)
            start(outward_sum(i, p))

        under(takes[i], add)

    def advance(core_lag, cross_lag):
        while len(to_core) > core_lag:
            job = to_core.pop(0)
            core_sum(*job)
            to_cross.append(job)
        while len(to_cross) > cross_lag:
            cross_sum(*to_cross.pop(0))

    def jobs(these):
        for job in these:
            down_step(*job)
            to_core.append(job)
            advance(2, 6)
        advance(0, 6)

    with jax.named_scope("fwd3"):
        dn_forward(nz - 1)
    with jax.named_scope("g_x"):
        from_x(0)
    if nz > 2:
        with jax.named_scope("g_z"):
            from_z(1)
        under(upper_inside, lambda: start(z_dn(2)))
    late = [nz - 1] if nz > 1 else []
    first_in = [0] + late
    rest = list(range(nz - 2, 0, -1))
    for i in range(2, nz - 1):
        with jax.named_scope("g_z"):
            under(inside, lambda i=i: from_z(i))
    local[6].wait()
    local[7].wait()
    with jax.named_scope("w_up"):
        for p in range(nz):
            from_y(p, up_out, uy_s, uy_r)
    with jax.named_scope("up"):
        up_step(0)
    for i in range(1, min(2, nz - 1)):
        with jax.named_scope("g_x"):
            from_x(i)
        with jax.named_scope("up"):
            up_step(i)
    with jax.named_scope("w_dn0"):
        for p in first_in:
            from_y(p, dn_out, dy_s, dy_r)
    with jax.named_scope("jobs"):
        jobs([(i, p) for i in range(min(2, nz - 1)) for p in first_in])
    for i in late:
        with jax.named_scope("g_z"):
            under(inside, lambda i=i: from_z(i))
    with jax.named_scope("fwd4"):
        for i in far_first[1:]:
            dn_forward(i)
    for i in range(2, nz):
        with jax.named_scope("g_z"):
            under(at_end, lambda i=i: from_z(i, False))
    for i in range(2, nz - 1):
        with jax.named_scope("g_x"):
            from_x(i)
        with jax.named_scope("up"):
            up_step(i)
        with jax.named_scope("jobs"):
            jobs([(i, p) for p in first_in])
    for p in rest:
        with jax.named_scope("w_dn"):
            from_y(p, dn_out, dy_s, dy_r)
        with jax.named_scope("jobs"):
            jobs([(i, p) for i in range(nz - 2, 0, -1)])
    for i in late:
        with jax.named_scope("g_x"):
            from_x(i)
        with jax.named_scope("up"):
            up_step(i)
        with jax.named_scope("jobs"):
            jobs([(i, p) for p in first_in + rest])
    outer_order = [1] + list(range(nz - 1, 1, -1)) + [0]
    with jax.named_scope("jobs"):
        jobs([(0, p) for p in rest])
    waiting = [(i, p) for i in range(2, nz - 1) for p in outer_order]
    with jax.named_scope("cross"):
        own_jobs = len([1 for job in to_cross if job[0] == 0])
        while len(to_cross) > own_jobs:
            advance(0, len(to_cross) - 1)
            if waiting:
                combine(*waiting.pop(0))
        for pair in waiting:
            combine(*pair)
    with jax.named_scope("comb3"):
        for i in range(max(nz - 1, 2), nz):
            for p in outer_order:
                combine(i, p)
    with jax.named_scope("cross_own"):
        advance(0, 0)
    with jax.named_scope("final"):
        group = zbuf.shape[3]
        for p in range(nz):
            for k in range(1, nz):
                slot = lambda: zbuf.at[turns[k], p]
                make = lambda: (slot(), slot(), cz_s.at[k, p], cz_r.at[turns[k], p], zabs[k])
                if k == 1:
                    arrive(make)
                    continue

                def nothing():
                    zbuf[turns[k], p] = jnp.zeros(zbuf.shape[2:], zbuf.dtype)

                pl.when(apart[k])(nothing)
                pl.when(jnp.logical_not(apart[k]))(lambda: arrive(make))
            ffn = after[:, p * group : (p + 1) * group].astype(jnp.float32)
            for a in range(nz):
                ffn = ffn + zbuf[a, p].astype(jnp.float32)
            out_ref[:, p * group : (p + 1) * group] = ffn.astype(jnp.bfloat16)

    with jax.named_scope("wait_send"):
        drain()


def layer(
    ny, nz, nx, q_lat, kv_lat, rope_key, cos, sin, q_gain, kv_gain, gain, resid,
    wqs, wql, wks, wkl, wos, wol, w_up, w_down,
):
    tp, sp = nx * CORES, ny * nz
    rows, width = resid.shape
    tok_rows, rank = kv_lat.shape
    small = wks.shape[1] // (2 * SMALL_DIM)
    large = wkl.shape[1] // (2 * LARGE_DIM)
    heads = small + large
    units = w_up.shape[1] // nz
    query_cols = -(-max(wqs.shape[0], wql.shape[0]) // LANES) * LANES
    dma = pltpu.SemaphoreType.DMA
    vmem = pl.BlockSpec(memory_space=pltpu.VMEM)
    anywhere = pl.BlockSpec(memory_space=pl.ANY)
    b16, f32 = jnp.bfloat16, jnp.float32

    def pair(*shape):
        return [dma(shape), dma(shape)]

    def like(array):
        return pltpu.VMEM(array.shape, array.dtype)

    return pl.pallas_call(
        functools.partial(layer_kernel, ny, nz, nx),
        out_shape=jax.ShapeDtypeStruct((rows, width), b16),
        in_specs=[vmem] * 9 + [anywhere] * 8,
        out_specs=vmem,
        scratch_shapes=[
            pltpu.VMEM((sp, tok_rows, rank + LANES), b16),
            pltpu.VMEM((sp, w_up.shape[0], units), b16),
            pltpu.VMEM((sp, units, w_down.shape[1]), b16),
            like(wqs),
            like(wql),
            like(wks),
            like(wkl),
            like(wos),
            like(wol),
            pltpu.VMEM((LANES, tok_rows), f32),
            pltpu.VMEM((tok_rows, query_cols), f32),
            pltpu.VMEM((heads, tok_rows, 2 * LANES), b16),
            pltpu.VMEM((heads, tok_rows, 1), f32),
            pltpu.VMEM((heads, tok_rows, 1), f32),
            pltpu.VMEM((heads, tok_rows, LARGE_DIM), f32),
            pltpu.VMEM((HALVES, CORES, nx, rows, width // HALVES), b16),
            pltpu.VMEM((HALVES, nx, rows, width // HALVES), b16),
            pltpu.VMEM((HALVES, nx, rows, width // HALVES), b16),
            pltpu.VMEM((rows, width), b16),
            pltpu.VMEM((nz, CORES, nx, rows, width), b16),
            pltpu.VMEM((nz, tp * rows, units), b16),
            pltpu.VMEM((nz, nz, CORES, nx, rows, width // nz), b16),
            pltpu.VMEM((nz, nz, nx, rows, width // nz), b16),
            pltpu.VMEM((nz, nz, nx, rows, width // nz), b16),
            pltpu.VMEM((nz, nz, rows, width // nz), b16),
            pltpu.VMEM((nz, nz, rows, width // nz), b16),
            pltpu.VMEM((nz, nz, rows, width // nz), b16),
            dma((8,)),
            pltpu.SemaphoreType.REGULAR,
        ]
        + pair(nz)
        + pair(nz, ny)
        + pair(nz, ny, nx) * 2
        + (pair(nz) + pair(nz, ny)) * 2
        + pair(HALVES)
        + pair(HALVES, nx)
        + pair(nz, HALVES)
        + [dma((HALVES,))]
        + pair(nz, nx, HALVES) * 2
        + pair(nz, nz)
        + pair(nz, nz, nx)
        + pair(nz, nz)
        + [dma((nz, nz))],
        compiler_params=pltpu.CompilerParams(
            collective_id=1, has_side_effects=True, vmem_limit_bytes=63 * 2**20
        ),
        name="layer",
    )(
        q_lat, kv_lat, rope_key, cos, sin, q_gain, kv_gain, gain, resid,
        wqs, wql, wks, wkl, wos, wol, w_up, w_down,
    )


def on_device(
    ny,
    nz,
    nx,
    resid,
    q_latent,
    kv_latent,
    rope_key,
    q_gain,
    kv_gain,
    w_q_small,
    w_q_large,
    w_kv_small,
    w_kv_large,
    w_out_small,
    w_out_large,
    ffn_gain,
    w_up,
    w_down,
):
    tok_rows = q_latent.shape[0]
    offset = lax.axis_index("sp") * tok_rows
    cos, sin = rotary_tables(offset + jnp.arange(tok_rows, dtype=jnp.int32))
    return layer(
        ny,
        nz,
        nx,
        q_latent,
        kv_latent,
        rope_key.T,
        cos,
        sin,
        q_gain.reshape(-1, LANES),
        kv_gain.reshape(1, -1),
        ffn_gain.reshape(1, -1),
        resid,
        w_q_small.T,
        w_q_large.T,
        w_kv_small,
        w_kv_large,
        w_out_small,
        w_out_large,
        w_up,
        w_down,
    )


def solution(mesh):
    ny = inner_split(mesh.shape["sp"])
    nz = mesh.shape["sp"] // ny
    nx = mesh.shape["tp"] // CORES
    return jax.shard_map(
        functools.partial(on_device, ny, nz, nx),
        mesh=mesh,
        in_specs=(
            P(("sp", "tp"), None),
            P("sp", None),
            P("sp", None),
            P("sp", None),
            P(),
            P(),
            P(None, "tp"),
            P(None, "tp"),
            P(None, "tp"),
            P(None, "tp"),
            P("tp", None),
            P("tp", None),
            P(),
            P("sp", "tp"),
            P("tp", "sp"),
        ),
        out_specs=P(("sp", "tp"), None),
        check_vma=False,
    )
```
